32 devices in a mesh: sp: 8 (over z, y), tp: 4 (over x, core).
Axes of the slice: x: 2, y: 2, z: 4, core: 2. Of those that a mesh axis runs over, the one named last changes fastest.
Arguments:
- proj_value: bfloat16 [4096, 2016], P('sp', 'tp'), may hold values from -6 to 6
- proj_gate: bfloat16 [4096, 2016], P('sp', 'tp'), may hold values from -8 to 8
- conv_saved: bfloat16 [4096, 2016], P('sp', 'tp'), may hold values from -12 to 12
- conv_taps: bfloat16 [31, 2016], P(None, 'tp'), may hold values from -1 to 1
- norm_gain: bfloat16 [2016], P('tp'), may hold values from 0.099609375 to 1.8984375
- out_weight: bfloat16 [2016, 2016], P('tp'), may hold values from -0.125 to 0.125
- cotangent: bfloat16 [4096, 2016], P('sp'), may hold values from -6 to 6
Outputs:
- grad_value: bfloat16 [4096, 2016], P('sp', 'tp')
- grad_gate: bfloat16 [4096, 2016], P('sp', 'tp')
- grad_out_weight: float32 [2016, 2016], P('tp', 'sp')
- grad_taps: float32 [31, 2016], P(None, 'tp')
The draws below stay inside these ranges and needn't reach their ends.
All inputs are finite; a program needn't handle non-finite values.
Results may differ from the reference program's by a relative error of at most 0.003.
Values sent between devices are 32-bit elements; how exact they have to be, the bound alone decides.
A program may use at most 64 MiB of HBM per device.

```python
import math
import jax
import jax.numpy as jnp
from jax import lax

D = 2016
KERNEL = 31
TOKENS = 4096


def draw_conv_saved(key, part):
    key_phase, key_rough, key_base = jax.random.split(jax.random.fold_in(key, 7), 3)
    channel = jnp.arange(D, dtype=jnp.float32) / D
    phase = jax.random.uniform(key_phase, (), jnp.float32, 0.0, 2.0 * math.pi)
    smooth = jnp.exp(1.2 * jnp.sin(2.0 * math.pi * 1.5 * channel + phase))
    rough = jnp.exp(jax.random.uniform(key_rough, (D,), jnp.float32, -0.4, 0.4))
    values = jax.random.normal(key_base, (TOKENS, D), jnp.float32) * smooth * rough
    return jnp.clip(values, -12.0, 12.0).astype(jnp.bfloat16)


def spiked(entries, stream_key, source, target, blocks, factor):
    owner, partner = [(jnp.arange(entries.shape[position]) // (entries.shape[position] // blocks)).reshape([-1 if axis == position else 1 for axis in range(entries.ndim)]) for position in (source, target)]
    chosen = jax.random.permutation(stream_key, blocks)[partner]
    strong = (owner == chosen) | (owner == (partner + blocks // 2) % blocks)
    return jnp.where(strong, factor * entries, entries)


def steps_of(key, extent, cuts, least, top_value):
    def one(position, parts):
        draws = jax.random.uniform(jax.random.fold_in(jax.random.fold_in(key, 6), position), (parts,), jnp.float32, least / len(cuts), top_value / len(cuts))
        return jnp.repeat(jnp.exp(draws), extent[position] // parts).reshape((-1,) + (1,) * (len(extent) - position - 1))

    loudness = one(*cuts[0])
    for cut in cuts[1:]:
        loudness = loudness * one(*cut)
    return loudness


def bell_draw(own_key, shape, deviation, bound, cuts=(), kind=jnp.bfloat16):
    drawn = jax.random.normal(own_key, shape, jnp.float32) * deviation
    if len(cuts) > 0:
        drawn = steps_of(own_key, shape, cuts, -0.22, 0.18) * drawn
    return jnp.clip(drawn, min=-bound, max=bound).astype(kind)


def heavy_noise(own_key, shape, width, limit, cuts, heavy, held_as=jnp.bfloat16):
    values = width * jax.random.normal(own_key, shape, jnp.float32)
    if cuts:
        values = values * steps_of(own_key, shape, cuts, -0.22, 0.18)
    return jnp.clip(spiked(values, jax.random.fold_in(own_key, 3), *heavy), -limit, limit).astype(held_as)


def setup_inputs(seed: int = 0) -> dict:
    arg_keys = jax.random.split(jax.random.key(seed), 8)
    return {
        "proj_value": bell_draw(arg_keys[0], (TOKENS, D), 1.0, 6.0, ((0, 8), (1, 4))),
        "proj_gate": bell_draw(arg_keys[1], (TOKENS, D), 1.5, 8.0, ((0, 8), (1, 4))),
        "conv_saved": draw_conv_saved(jax.random.fold_in(arg_keys[7], 71), 0),
        "conv_taps": bell_draw(arg_keys[3], (KERNEL, D), KERNEL ** -0.5, 1.0, ((1, 4),)),
        "norm_gain": jnp.clip(1.0 + 0.18 * jax.random.normal(arg_keys[4], (D,), jnp.float32), 0.099609375, 1.8984375).astype(jnp.bfloat16),
        "out_weight": bell_draw(arg_keys[5], (D, D), D ** -0.5, 0.125, ((0, 4),)),
        "cotangent": heavy_noise(arg_keys[6], (TOKENS, D), 1.0, 6.0, ((0, 8),), (0, 1, 8, 2.0)),
    }


norm_eps = 1e-05

def reference(proj_value, proj_gate, conv_saved, conv_taps, norm_gain, out_weight, cotangent):
    conv_f = conv_saved.astype(jnp.float32)
    row_mean = lax.optimization_barrier(jnp.sum(conv_f, axis=1)) / D
    row_var = lax.optimization_barrier(jnp.sum(conv_f * conv_f, axis=1)) / D - row_mean * row_mean
    inv_std = lax.rsqrt(row_var + norm_eps)
    centered = (conv_f - row_mean[:, None]) * inv_std[:, None]
    gain_f = norm_gain.astype(jnp.float32)
    normed = centered * gain_f
    gate_norm = jax.nn.sigmoid(normed)
    activated = (normed * gate_norm).astype(jnp.bfloat16)
    grad_scale = 1.0 / math.sqrt(TOKENS)
    grad_out_weight = jnp.dot(activated.T, cotangent, preferred_element_type=jnp.float32) * grad_scale
    d_act = jnp.dot(cotangent, out_weight.T, preferred_element_type=jnp.float32)
    d_hat = d_act * gate_norm * (1.0 + normed * (1.0 - gate_norm)) * gain_f
    first = lax.optimization_barrier(jnp.sum(d_hat, axis=1)) / D
    second = lax.optimization_barrier(jnp.sum(d_hat * centered, axis=1)) / D
    d_conv = inv_std[:, None] * (d_hat - first[:, None] - centered * second[:, None])
    overhang = KERNEL - 1
    extended = jnp.concatenate([d_conv, jnp.zeros((overhang, D), jnp.float32)], axis=0)
    gate_proj = jax.nn.sigmoid(proj_gate.astype(jnp.float32))
    gated = proj_value.astype(jnp.float32) * gate_proj
    taps_f = conv_taps.astype(jnp.float32)
    d_glu = jnp.zeros((TOKENS, D), jnp.float32)
    tap_rows = []
    for offset in range(KERNEL):
        shifted = extended[overhang - offset:overhang - offset + TOKENS]
        d_glu = d_glu + taps_f[offset] * shifted
        tap_rows.append(lax.optimization_barrier(jnp.sum(gated * shifted, axis=0)))
    grad_taps = jnp.stack(tap_rows) * grad_scale
    grad_value = (d_glu * gate_proj).astype(jnp.bfloat16)
    grad_gate = (d_glu * gated * (1.0 - gate_proj)).astype(jnp.bfloat16)
    return (grad_value, grad_gate, grad_out_weight, grad_taps)
```

```python
import functools
import math

import jax
import jax.numpy as jnp
from jax import lax
from jax.experimental import pallas as pl
from jax.experimental.pallas import tpu as pltpu
from jax.sharding import PartitionSpec as P

norm_eps = 1e-05
MESH = pl.DeviceIdType.MESH
f32 = jnp.float32


def line_order(length):
    rows = []
    for place in range(length):
        side = 1 if 2 * place >= length else -1
        rows.append(sorted(range(length), key=lambda d: (-abs(d - place), -side * (d - place))))
    return rows


def lookup(table, place):
    value = table[0]
    for i in range(1, len(table)):
        value = jnp.where(place == i, table[i], value)
    return value


def kernel(
    n_sp, n_tp, fold, pv, pg, conv, taps, gain, weight, cot,
    out_v, out_g, out_w, out_t,
    act_t, d_act, ext, shifted, cols, cols2, term, got_y, got_r, got_l,
    stat, stat_in, mom, mom_in, grad_acc, g_own, g_mid, g_in, g_yin, taps_b,
    stat_ss, stat_rs, mom_ss, mom_rs, y_ss, y_rs, r_ss, r_rs, l_ss, l_rs,
    halo_ss, halo_rs, gz_ss, gz_rs, gy_ss, gy_rs,
):
    s = lax.axis_index("sp")
    t = lax.axis_index("tp")
    n_z = n_sp // fold
    z = s // fold
    y = s % fold
    other_y = 1 - y
    rows, width = cot.shape
    ch = conv.shape[1]
    part = out_w.shape[1]
    n_taps = taps.shape[0]
    scale = 1.0 / math.sqrt(rows * n_sp)
    blk = 128
    n_blk = rows // blk

    barrier = pltpu.get_barrier_semaphore()
    for i in range(1, n_sp):
        pl.semaphore_signal(barrier, inc=1, device_id=(lax.rem(s + i, n_sp), t), device_id_type=MESH)
    for i in range(1, n_tp):
        pl.semaphore_signal(barrier, inc=1, device_id=(s, lax.rem(t + i, n_tp)), device_id_type=MESH)

    def pack(a, b):
        lane = lax.broadcasted_iota(jnp.int32, (blk, blk), 1)
        return jnp.where(lane == 0, a, b).T[:8]

    def unpack(x):
        return jnp.concatenate([x] * (blk // 8), axis=0).T

    @pl.loop(0, n_blk)
    def _(i):
        at = pl.ds(pl.multiple_of(i * blk, blk), blk)
        c = conv[at, :].astype(f32)
        stat[:, at] = pack(jnp.sum(c, axis=1, keepdims=True), jnp.sum(c * c, axis=1, keepdims=True))

    pl.semaphore_wait(barrier, n_sp - 1 + n_tp - 1)

    def tp_copies(src, dst, ss, rs):
        return [
            pltpu.make_async_remote_copy(
                src_ref=src, dst_ref=dst.at[i - 1], send_sem=ss.at[i - 1], recv_sem=rs.at[i - 1],
                device_id=(s, lax.rem(t + i, n_tp)), device_id_type=MESH,
            )
            for i in range(1, n_tp)
        ]

    stat_copies = tp_copies(stat, stat_in, stat_ss, stat_rs)
    for c in stat_copies:
        c.start()

    @pl.loop(0, n_blk)
    def _(i):
        at = pl.ds(pl.multiple_of(i * blk, blk), blk)
        d_act[at, :] = lax.dot_general(
            cot[at, :], weight[...], (((1,), (1,)), ((), ())), preferred_element_type=f32
        )

    for c in stat_copies:
        c.wait()
    total = stat[...]
    for i in range(n_tp - 1):
        total = total + stat_in[i]
    mean = total[0:1] / width
    inv = lax.rsqrt(total[1:2] / width - mean * mean + norm_eps)
    row8 = lax.broadcasted_iota(jnp.int32, (8, rows), 0)
    both = jnp.where(row8 == 0, mean, inv)
    for i in range(n_blk):
        cols[i * blk:(i + 1) * blk, :] = unpack(both[:, i * blk:(i + 1) * blk])

    gain_f = gain[...].astype(f32)

    @pl.loop(0, n_blk)
    def _(i):
        at = pl.ds(pl.multiple_of(i * blk, blk), blk)
        c = conv[at, :].astype(f32)
        normed = (c - cols[at, 0:1]) * cols[at, 1:2] * gain_f
        a = normed * jax.nn.sigmoid(normed)
        act_t[:, at] = a.T.astype(jnp.bfloat16)

    for j in range(n_sp):
        term[j] = jnp.dot(act_t[...], cot[:, j * part:(j + 1) * part], preferred_element_type=f32)

    orders = line_order(n_z)
    dest = [lookup([orders[i][k] for i in range(n_z)], z) for k in range(n_z)]

    def y_copy(k):
        return pltpu.make_async_remote_copy(
            src_ref=term.at[dest[k] * fold + other_y], dst_ref=got_y.at[dest[k]],
            send_sem=y_ss.at[dest[k]], recv_sem=y_rs.at[dest[k]],
            device_id=(z * fold + other_y, t), device_id_type=MESH,
        )

    y_copies = [y_copy(k) for k in range(n_z)]

    def line_copy(d, up):
        buf, ss, rs = (got_r, r_ss, r_rs) if up else (got_l, l_ss, l_rs)
        to = z + 1 if up else z - 1
        to = jnp.clip(to, 0, n_z - 1)
        return pltpu.make_async_remote_copy(
            src_ref=term.at[d * fold + y], dst_ref=buf.at[d], send_sem=ss.at[d], recv_sem=rs.at[d],
            device_id=(to * fold + y, t), device_id_type=MESH,
        )

    def add_into(d, buf):
        own = d * fold + y
        step = 56 if ch % 56 == 0 else 8

        @pl.loop(0, ch // step)
        def _(i):
            at = pl.ds(pl.multiple_of(i * step, 8), step)
            term[own, at, :] = term[own, at, :] + buf[d, at, :]

    def hop(k):
        d = dest[k]
        y_copies[k].wait_recv()
        add_into(d, got_y)

        @pl.when(d > z)
        def _():
            @pl.when(z > 0)
            def _():
                line_copy(d, True).wait_recv()
                add_into(d, got_r)

            line_copy(d, True).start()

        @pl.when(d < z)
        def _():
            @pl.when(z < n_z - 1)
            def _():
                line_copy(d, False).wait_recv()
                add_into(d, got_l)

            line_copy(d, False).start()

    y_copies[0].start()
    y_copies[1].start()

    @pl.loop(0, n_blk)
    def _(i):
        at = pl.ds(pl.multiple_of(i * blk, blk), blk)
        c = conv[at, :].astype(f32)
        centered = (c - cols[at, 0:1]) * cols[at, 1:2]
        normed = centered * gain_f
        gate = jax.nn.sigmoid(normed)
        d_hat = d_act[at, :] * gate * (1.0 + normed * (1.0 - gate)) * gain_f
        d_act[at, :] = d_hat
        mom[:, at] = pack(
            jnp.sum(d_hat, axis=1, keepdims=True), jnp.sum(d_hat * centered, axis=1, keepdims=True)
        )

    mom_copies = tp_copies(mom, mom_in, mom_ss, mom_rs)
    for c in mom_copies:
        c.start()
    for k in range(n_taps):
        taps_b[k] = jnp.broadcast_to(taps[k:k + 1, :].astype(f32), (8, ch))
    grad_acc[...] = jnp.zeros_like(grad_acc)
    for c in mom_copies:
        c.wait()
    total = mom[...]
    for i in range(n_tp - 1):
        total = total + mom_in[i]
    total = total / width
    for i in range(n_blk):
        cols2[i * blk:(i + 1) * blk, :] = unpack(total[:, i * blk:(i + 1) * blk])

    @pl.loop(0, n_blk)
    def _(i):
        at = pl.ds(pl.multiple_of(i * blk, blk), blk)
        c = conv[at, :].astype(f32)
        inv_std = cols[at, 1:2]
        centered = (c - cols[at, 0:1]) * inv_std
        ext[at, :] = inv_std * (d_act[at, :] - cols2[at, 0:1] - centered * cols2[at, 1:2])

    reach = 32
    back = jnp.maximum(s - 1, 0)
    halo = pltpu.make_async_remote_copy(
        src_ref=ext.at[pl.ds(0, reach), :], dst_ref=ext.at[pl.ds(rows, reach), :],
        send_sem=halo_ss, recv_sem=halo_rs, device_id=(back, t), device_id_type=MESH,
    )

    @pl.when(s > 0)
    def _():
        halo.start()

    for k in range(2, n_z):
        y_copies[k].start()

    def shift_block(i):
        start = pl.multiple_of(i * reach, reach)
        win = ext[pl.ds(start, reach + 8), :]
        for o in range(8):
            shifted[o, pl.ds(start, reach), :] = win[o:o + reach]

    lanes = [(lo, min(128, ch - lo)) for lo in range(0, ch, 128)]

    def conv_blocks(first, last):
        for lo, wide in lanes:
            ln = slice(lo, lo + wide)

            def body(i, accs):
                start = pl.multiple_of(i * reach, reach)
                at = pl.ds(start, reach)
                gate = jax.nn.sigmoid(pg[at, ln].astype(f32))
                gated = pv[at, ln].astype(f32) * gate
                d_glu = jnp.zeros((reach, wide), f32)
                out = []
                for o in range(n_taps):
                    x = shifted[o % 8, pl.ds(pl.multiple_of(start + 8 * (o // 8), 8), reach), ln]
                    tap = taps_b[n_taps - 1 - o, :, ln]
                    d_glu = d_glu + jnp.concatenate([tap] * (reach // 8), axis=0) * x
                    prod = gated * x
                    acc = accs[o]
                    for q in range(reach // 8):
                        acc = acc + prod[8 * q:8 * q + 8]
                    out.append(acc)
                out_v[at, ln] = (d_glu * gate).astype(jnp.bfloat16)
                out_g[at, ln] = (d_glu * gated * (1.0 - gate)).astype(jnp.bfloat16)
                return tuple(out)

            accs = tuple(grad_acc[n_taps - 1 - o, :, ln] for o in range(n_taps))
            accs = lax.fori_loop(first, last, body, accs)
            for o in range(n_taps):
                grad_acc[n_taps - 1 - o, :, ln] = accs[o]

    n_row = rows // reach

    @pl.loop(0, n_row - 1)
    def _(i):
        shift_block(i)

    hop(0)
    half = (n_row - 2) // 2
    conv_blocks(0, half)
    hop(1)
    conv_blocks(half, n_row - 2)

    @pl.when(s < n_sp - 1)
    def _():
        halo.wait_recv()

    @pl.when(s == n_sp - 1)
    def _():
        ext[pl.ds(rows, reach), :] = jnp.zeros((reach, ch), f32)

    shift_block(n_row - 1)
    win = ext[pl.ds(rows, reach), :]
    for o in range(8):
        shifted[o, pl.ds(rows, reach - 8), :] = win[o:o + reach - 8]
    conv_blocks(n_row - 2, n_row)

    for k in range(n_taps):
        g_own[k:k + 1, :] = jnp.sum(grad_acc[k], axis=0, keepdims=True)
    for k in range(n_taps, g_own.shape[0]):
        g_own[k:k + 1, :] = jnp.zeros((1, ch), f32)
    gz_copies = [
        pltpu.make_async_remote_copy(
            src_ref=g_own, dst_ref=g_in.at[i - 1], send_sem=gz_ss.at[i - 1], recv_sem=gz_rs.at[i - 1],
            device_id=(lax.rem(z + i, n_z) * fold + y, t), device_id_type=MESH,
        )
        for i in range(1, n_z)
    ]
    for c in gz_copies:
        c.start()
    for k in range(2, n_z - 1):
        hop(k)
    for c in gz_copies:
        c.wait()
    total = g_own[...]
    for i in range(n_z - 1):
        total = total + g_in[i]
    g_mid[...] = total
    gy = pltpu.make_async_remote_copy(
        src_ref=g_mid, dst_ref=g_yin, send_sem=gy_ss, recv_sem=gy_rs,
        device_id=(z * fold + other_y, t), device_id_type=MESH,
    )
    gy.start()
    y_copies[n_z - 1].wait_recv()
    add_into(z, got_y)

    @pl.when(z > 0)
    def _():
        line_copy(z, True).wait_recv()
        add_into(z, got_r)

    @pl.when(z < n_z - 1)
    def _():
        line_copy(z, False).wait_recv()
        add_into(z, got_l)

    out_w[...] = term[z * fold + y] * scale
    gy.wait()
    out_t[...] = ((g_mid[...] + g_yin[...]) * scale)[:n_taps]
    for k in range(n_z):
        y_copies[k].wait_send()

    @pl.when(s > 0)
    def _():
        halo.wait_send()

    for k in range(n_z - 1):
        d = dest[k]

        @pl.when(d > z)
        def _():
            line_copy(d, True).wait_send()

        @pl.when(d < z)
        def _():
            line_copy(d, False).wait_send()


def fused(n_sp, n_tp, proj_value, proj_gate, conv_saved, conv_taps, norm_gain, out_weight, cotangent):
    fold = 2
    n_z = n_sp // fold
    rows, width = cotangent.shape
    ch = conv_saved.shape[1]
    n_taps = conv_taps.shape[0]
    part = width // n_sp
    dma = pltpu.SemaphoreType.DMA
    V = pltpu.VMEM
    bf = jnp.bfloat16
    vm = pl.BlockSpec(memory_space=pltpu.VMEM)
    return pl.pallas_call(
        functools.partial(kernel, n_sp, n_tp, fold),
        out_shape=(
            jax.ShapeDtypeStruct((rows, ch), bf),
            jax.ShapeDtypeStruct((rows, ch), bf),
            jax.ShapeDtypeStruct((ch, part), f32),
            jax.ShapeDtypeStruct((n_taps, ch), f32),
        ),
        in_specs=[vm] * 7,
        out_specs=[vm] * 4,
        scratch_shapes=[
            V((ch, rows), bf), V((rows, ch), f32), V((rows + 32, ch), f32), V((8, rows + 32, ch), f32),
            V((rows, 128), f32), V((rows, 128), f32),
            V((n_sp, ch, part), f32), V((n_z, ch, part), f32), V((n_z, ch, part), f32),
            V((n_z, ch, part), f32),
            V((8, rows), f32), V((n_tp - 1, 8, rows), f32), V((8, rows), f32), V((n_tp - 1, 8, rows), f32),
            V((n_taps, 8, ch), f32), V((32, ch), f32), V((32, ch), f32), V((n_z - 1, 32, ch), f32),
            V((32, ch), f32), V((n_taps, 8, ch), f32),
            dma((n_tp - 1,)), dma((n_tp - 1,)), dma((n_tp - 1,)), dma((n_tp - 1,)),
            dma((n_z,)), dma((n_z,)), dma((n_z,)), dma((n_z,)), dma((n_z,)), dma((n_z,)),
            dma, dma, dma((n_z - 1,)), dma((n_z - 1,)), dma, dma,
        ],
        compiler_params=pltpu.CompilerParams(
            collective_id=0, has_side_effects=True, vmem_limit_bytes=60 * 1024 * 1024
        ),
    )(proj_value, proj_gate, conv_saved, conv_taps, norm_gain.reshape(1, ch), out_weight, cotangent)


def passed_along(block, axis, distance):
    devices = range(lax.axis_size(axis))
    route = [(i - distance, i) for i in devices if i - distance in devices]
    return lax.ppermute(block, axis, route)


def local(proj_value, proj_gate, conv_saved, conv_taps, norm_gain, out_weight, cotangent):
    model_width = cotangent.shape[1]
    tok_rows = cotangent.shape[0]
    tap_count = conv_taps.shape[0]
    overhang = tap_count - 1
    grad_scale = 1.0 / math.sqrt(tok_rows * lax.axis_size("sp"))
    conv_f = conv_saved.astype(jnp.float32)
    totals = lax.psum((jnp.sum(conv_f, axis=1), jnp.sum(conv_f * conv_f, axis=1)), "tp")
    row_mean = totals[0] / model_width
    row_var = totals[1] / model_width - row_mean * row_mean
    inv_std = lax.rsqrt(row_var + norm_eps)
    centered = (conv_f - row_mean[:, None]) * inv_std[:, None]
    gain_f = norm_gain.astype(jnp.float32)
    normed = centered * gain_f
    gate_norm = jax.nn.sigmoid(normed)
    activated = (normed * gate_norm).astype(jnp.bfloat16)
    contract_rows = (((0,), (0,)), ((), ()))
    whole_term = lax.dot_general(
        cotangent, activated, contract_rows, preferred_element_type=jnp.float32
    )
    shard_grad = lax.psum_scatter(whole_term, "sp", scatter_dimension=0, tiled=True)
    grad_out_weight = shard_grad.T * grad_scale
    d_act = lax.dot_general(
        cotangent, out_weight, (((1,), (1,)), ((), ())), preferred_element_type=jnp.float32
    )
    d_hat = d_act * gate_norm * (1.0 + normed * (1.0 - gate_norm)) * gain_f
    moments = lax.psum((jnp.sum(d_hat, axis=1), jnp.sum(d_hat * centered, axis=1)), "tp")
    first = moments[0] / model_width
    second = moments[1] / model_width
    d_conv = inv_std[:, None] * (d_hat - first[:, None] - centered * second[:, None])
    ahead = passed_along(d_conv[:overhang], "sp", -1)
    extended = jnp.concatenate([d_conv, ahead], axis=0)
    gate_proj = jax.nn.sigmoid(proj_gate.astype(jnp.float32))
    gated = proj_value.astype(jnp.float32) * gate_proj
    taps_f = conv_taps.astype(jnp.float32)
    d_glu = jnp.zeros_like(d_conv)
    tap_rows = []
    for offset in range(tap_count):
        shifted = extended[overhang - offset : overhang - offset + tok_rows]
        d_glu = d_glu + taps_f[offset] * shifted
        tap_rows.append(jnp.sum(gated * shifted, axis=0))
    grad_taps = lax.psum(jnp.stack(tap_rows), "sp") * grad_scale
    grad_value = (d_glu * gate_proj).astype(jnp.bfloat16)
    grad_gate = (d_glu * gated * (1.0 - gate_proj)).astype(jnp.bfloat16)
    return (grad_value, grad_gate, grad_out_weight, grad_taps)


def solution(mesh):
    in_specs = (
        P("sp", "tp"),
        P("sp", "tp"),
        P("sp", "tp"),
        P(None, "tp"),
        P("tp"),
        P("tp", None),
        P("sp", None),
    )
    out_specs = (P("sp", "tp"), P("sp", "tp"), P("tp", "sp"), P(None, "tp"))
    n_sp, n_tp = mesh.shape["sp"], mesh.shape["tp"]

    def step(*args):
        rows, width = args[6].shape
        ch, n_taps = args[2].shape[1], args[3].shape[0]
        small = n_sp % 2 == 0 and 4 <= n_sp <= 8 and width % n_sp == 0 and n_tp > 1
        if small and rows % 128 == 0 and rows >= 128 and ch % 8 == 0 and 24 < n_taps <= 31:
            return fused(n_sp, n_tp, *args)
        return local(*args)

    return jax.shard_map(step, mesh=mesh, in_specs=in_specs, out_specs=out_specs, check_vma=False)
```

```python
import functools
import math

import jax
import jax.numpy as jnp
from jax import lax
from jax.experimental import pallas as pl
from jax.experimental.pallas import tpu as pltpu
from jax.sharding import PartitionSpec as P

norm_eps = 1e-05
MESH = pl.DeviceIdType.MESH
f32 = jnp.float32


def line_order(length):
    rows = []
    for place in range(length):
        side = 1 if 2 * place >= length else -1
        rows.append(sorted(range(length), key=lambda d: (-abs(d - place), -side * (d - place))))
    return rows


def lookup(table, place):
    value = table[0]
    for i in range(1, len(table)):
        value = jnp.where(place == i, table[i], value)
    return value


def kernel(
    n_sp, n_tp, fold, pv_h, pg_h, conv, taps, gain, weight_h, cot_h,
    out_v, out_g, out_w, out_t,
    pv, pg, weight, cot, in_sems, gain_c, gated_s, d_glu_s, act_t, d_act, ext, shifted, cols, cols2, term, got_y, got_r, got_l,
    stat, stat_in, mom, mom_in, grad_acc, g_own, g_mid, g_in, g_yin, taps_b,
    stat_ss, stat_rs, mom_ss, mom_rs, y_ss, y_rs, r_ss, r_rs, l_ss, l_rs,
    halo_ss, halo_rs, gz_ss, gz_rs, gy_ss, gy_rs,
):
    s = lax.axis_index("sp")
    t = lax.axis_index("tp")
    n_z = n_sp // fold
    z = s // fold
    y = s % fold
    other_y = 1 - y
    width, rows = cot.shape
    ch = conv.shape[0]
    part = out_w.shape[1]
    n_taps = taps.shape[0]
    scale = 1.0 / math.sqrt(rows * n_sp)
    blk = 128
    n_blk = rows // blk

    loads = [
        pltpu.make_async_copy(a, b, in_sems.at[i])
        for i, (a, b) in enumerate([(cot_h, cot), (weight_h, weight), (pv_h, pv), (pg_h, pg)])
    ]
    for c in loads:
        c.start()

    barrier = pltpu.get_barrier_semaphore()
    for i in range(1, n_sp):
        pl.semaphore_signal(barrier, inc=1, device_id=(lax.rem(s + i, n_sp), t), device_id_type=MESH)
    for i in range(1, n_tp):
        pl.semaphore_signal(barrier, inc=1, device_id=(s, lax.rem(t + i, n_tp)), device_id_type=MESH)

    row8b = lax.broadcasted_iota(jnp.int32, (8, blk), 0)

    @pl.loop(0, n_blk)
    def _(i):
        at = pl.ds(pl.multiple_of(i * blk, blk), blk)
        c = conv[:, at].astype(f32)
        stat[:, at] = jnp.where(
            row8b == 0, jnp.sum(c, axis=0, keepdims=True), jnp.sum(c * c, axis=0, keepdims=True)
        )

    pl.semaphore_wait(barrier, n_sp - 1 + n_tp - 1)

    def tp_copies(src, dst, ss, rs):
        return [
            pltpu.make_async_remote_copy(
                src_ref=src, dst_ref=dst.at[i - 1], send_sem=ss.at[i - 1], recv_sem=rs.at[i - 1],
                device_id=(s, lax.rem(t + i, n_tp)), device_id_type=MESH,
            )
            for i in range(1, n_tp)
        ]

    stat_copies = tp_copies(stat, stat_in, stat_ss, stat_rs)
    for c in stat_copies:
        c.start()

    gain_c[...] = jnp.broadcast_to(gain[...].astype(f32), (128, ch)).T
    loads[0].wait()
    loads[1].wait()
    wide_blk = 256 if rows % 256 == 0 else 128

    @pl.loop(0, rows // wide_blk)
    def _(i):
        at = pl.ds(pl.multiple_of(i * wide_blk, wide_blk), wide_blk)
        d_act[:, at] = jnp.dot(weight[...], cot[:, at], preferred_element_type=f32)

    for c in stat_copies:
        c.wait()
    total = stat[...]
    for i in range(n_tp - 1):
        total = total + stat_in[i]
    mean = total[0:1] / width
    inv = lax.rsqrt(total[1:2] / width - mean * mean + norm_eps)
    row8 = lax.broadcasted_iota(jnp.int32, (8, rows), 0)
    cols[...] = jnp.where(row8 == 0, mean, inv)

    @pl.loop(0, n_blk)
    def _(i):
        at = pl.ds(pl.multiple_of(i * blk, blk), blk)
        c = conv[:, at].astype(f32)
        normed = (c - cols[0:1, at]) * cols[1:2, at] * gain_c[...]
        act_t[:, at] = (normed * jax.nn.sigmoid(normed)).astype(jnp.bfloat16)

    for j in range(n_sp):
        term[j] = lax.dot_general(
            act_t[...], cot[j * part:(j + 1) * part, :], (((1,), (1,)), ((), ())),
            preferred_element_type=f32,
        )

    orders = line_order(n_z)
    dest = [lookup([orders[i][k] for i in range(n_z)], z) for k in range(n_z)]

    def y_copy(k):
        return pltpu.make_async_remote_copy(
            src_ref=term.at[dest[k] * fold + other_y], dst_ref=got_y.at[dest[k]],
            send_sem=y_ss.at[dest[k]], recv_sem=y_rs.at[dest[k]],
            device_id=(z * fold + other_y, t), device_id_type=MESH,
        )

    y_copies = [y_copy(k) for k in range(n_z)]

    def line_copy(d, up):
        buf, ss, rs = (got_r, r_ss, r_rs) if up else (got_l, l_ss, l_rs)
        to = z + 1 if up else z - 1
        to = jnp.clip(to, 0, n_z - 1)
        return pltpu.make_async_remote_copy(
            src_ref=term.at[d * fold + y], dst_ref=buf.at[d], send_sem=ss.at[d], recv_sem=rs.at[d],
            device_id=(to * fold + y, t), device_id_type=MESH,
        )

    def add_into(d, buf):
        own = d * fold + y
        step = 56 if ch % 56 == 0 else 8

        @pl.loop(0, ch // step)
        def _(i):
            at = pl.ds(pl.multiple_of(i * step, 8), step)
            term[own, at, :] = term[own, at, :] + buf[d, at, :]

    def hop(k):
        d = dest[k]
        y_copies[k].wait_recv()
        add_into(d, got_y)

        @pl.when(d > z)
        def _():
            @pl.when(z > 0)
            def _():
                line_copy(d, True).wait_recv()
                add_into(d, got_r)

            line_copy(d, True).start()

        @pl.when(d < z)
        def _():
            @pl.when(z < n_z - 1)
            def _():
                line_copy(d, False).wait_recv()
                add_into(d, got_l)

            line_copy(d, False).start()

    y_copies[0].start()
    y_copies[1].start()

    @pl.loop(0, n_blk)
    def _(i):
        at = pl.ds(pl.multiple_of(i * blk, blk), blk)
        c = conv[:, at].astype(f32)
        centered = (c - cols[0:1, at]) * cols[1:2, at]
        normed = centered * gain_c[...]
        gate = jax.nn.sigmoid(normed)
        d_hat = d_act[:, at] * gate * (1.0 + normed * (1.0 - gate)) * gain_c[...]
        d_act[:, at] = d_hat
        mom[:, at] = jnp.where(
            row8b == 0, jnp.sum(d_hat, axis=0, keepdims=True),
            jnp.sum(d_hat * centered, axis=0, keepdims=True),
        )

    mom_copies = tp_copies(mom, mom_in, mom_ss, mom_rs)
    for c in mom_copies:
        c.start()
    for k in range(n_taps):
        taps_b[k] = jnp.broadcast_to(taps[k:k + 1, :].astype(f32), (8, ch))
    grad_acc[...] = jnp.zeros_like(grad_acc)
    loads[2].wait()
    loads[3].wait()

    @pl.loop(0, n_blk)
    def _(i):
        at = pl.ds(pl.multiple_of(i * blk, blk), blk)
        gated_s[at, :] = (pv[:, at].astype(f32) * jax.nn.sigmoid(pg[:, at].astype(f32))).T

    for c in mom_copies:
        c.wait()
    total = mom[...]
    for i in range(n_tp - 1):
        total = total + mom_in[i]
    cols2[...] = total / width

    @pl.loop(0, n_blk)
    def _(i):
        at = pl.ds(pl.multiple_of(i * blk, blk), blk)
        c = conv[:, at].astype(f32)
        inv_std = cols[1:2, at]
        centered = (c - cols[0:1, at]) * inv_std
        ext[at, :] = (inv_std * (d_act[:, at] - cols2[0:1, at] - centered * cols2[1:2, at])).T

    reach = 32
    back = jnp.maximum(s - 1, 0)
    halo = pltpu.make_async_remote_copy(
        src_ref=ext.at[pl.ds(0, reach), :], dst_ref=ext.at[pl.ds(rows, reach), :],
        send_sem=halo_ss, recv_sem=halo_rs, device_id=(back, t), device_id_type=MESH,
    )

    @pl.when(s > 0)
    def _():
        halo.start()

    for k in range(2, n_z):
        y_copies[k].start()

    def shift_block(i):
        start = pl.multiple_of(i * reach, reach)
        win = ext[pl.ds(start, reach + 8), :]
        for o in range(8):
            shifted[o, pl.ds(start, reach), :] = win[o:o + reach]

    lanes = [(lo, min(128, ch - lo)) for lo in range(0, ch, 128)]

    def conv_blocks(first, last):
        for lo, wide in lanes:
            ln = slice(lo, lo + wide)

            def body(i, accs):
                start = pl.multiple_of(i * reach, reach)
                at = pl.ds(start, reach)
                gated = gated_s[at, ln]
                d_glu = jnp.zeros((reach, wide), f32)
                out = []
                for o in range(n_taps):
                    x = shifted[o % 8, pl.ds(pl.multiple_of(start + 8 * (o // 8), 8), reach), ln]
                    tap = taps_b[n_taps - 1 - o, :, ln]
                    d_glu = d_glu + jnp.concatenate([tap] * (reach // 8), axis=0) * x
                    prod = gated * x
                    acc = accs[o]
                    for q in range(reach // 8):
                        acc = acc + prod[8 * q:8 * q + 8]
                    out.append(acc)
                d_glu_s[at, ln] = d_glu
                return tuple(out)

            accs = tuple(grad_acc[n_taps - 1 - o, :, ln] for o in range(n_taps))
            accs = lax.fori_loop(first, last, body, accs)
            for o in range(n_taps):
                grad_acc[n_taps - 1 - o, :, ln] = accs[o]

    n_row = rows // reach

    @pl.loop(0, n_row - 1)
    def _(i):
        shift_block(i)

    hop(0)
    half = (n_row - 2) // 2
    conv_blocks(0, half)
    hop(1)
    conv_blocks(half, n_row - 2)

    @pl.when(s < n_sp - 1)
    def _():
        halo.wait_recv()

    @pl.when(s == n_sp - 1)
    def _():
        ext[pl.ds(rows, reach), :] = jnp.zeros((reach, ch), f32)

    shift_block(n_row - 1)
    win = ext[pl.ds(rows, reach), :]
    for o in range(8):
        shifted[o, pl.ds(rows, reach - 8), :] = win[o:o + reach - 8]
    conv_blocks(n_row - 2, n_row)

    for k in range(n_taps):
        g_own[k:k + 1, :] = jnp.sum(grad_acc[k], axis=0, keepdims=True)
    for k in range(n_taps, g_own.shape[0]):
        g_own[k:k + 1, :] = jnp.zeros((1, ch), f32)
    gz_copies = [
        pltpu.make_async_remote_copy(
            src_ref=g_own, dst_ref=g_in.at[i - 1], send_sem=gz_ss.at[i - 1], recv_sem=gz_rs.at[i - 1],
            device_id=(lax.rem(z + i, n_z) * fold + y, t), device_id_type=MESH,
        )
        for i in range(1, n_z)
    ]
    for c in gz_copies:
        c.start()
    for k in range(2, n_z - 1):
        hop(k)

    @pl.loop(0, n_blk)
    def _(i):
        at = pl.ds(pl.multiple_of(i * blk, blk), blk)
        gate = jax.nn.sigmoid(pg[:, at].astype(f32))
        d_glu = d_glu_s[at, :].T
        out_v[:, at] = (d_glu * gate).astype(jnp.bfloat16)
        out_g[:, at] = (d_glu * (pv[:, at].astype(f32) * gate) * (1.0 - gate)).astype(jnp.bfloat16)

    for c in gz_copies:
        c.wait()
    total = g_own[...]
    for i in range(n_z - 1):
        total = total + g_in[i]
    g_mid[...] = total
    gy = pltpu.make_async_remote_copy(
        src_ref=g_mid, dst_ref=g_yin, send_sem=gy_ss, recv_sem=gy_rs,
        device_id=(z * fold + other_y, t), device_id_type=MESH,
    )
    gy.start()
    y_copies[n_z - 1].wait_recv()
    add_into(z, got_y)

    @pl.when(z > 0)
    def _():
        line_copy(z, True).wait_recv()
        add_into(z, got_r)

    @pl.when(z < n_z - 1)
    def _():
        line_copy(z, False).wait_recv()
        add_into(z, got_l)

    out_w[...] = term[z * fold + y] * scale
    gy.wait()
    out_t[...] = ((g_mid[...] + g_yin[...]) * scale)[:n_taps]
    for k in range(n_z):
        y_copies[k].wait_send()

    @pl.when(s > 0)
    def _():
        halo.wait_send()

    for k in range(n_z - 1):
        d = dest[k]

        @pl.when(d > z)
        def _():
            line_copy(d, True).wait_send()

        @pl.when(d < z)
        def _():
            line_copy(d, False).wait_send()


def fused(n_sp, n_tp, proj_value, proj_gate, conv_saved, conv_taps, norm_gain, out_weight, cotangent):
    fold = 2
    n_z = n_sp // fold
    rows, width = cotangent.shape
    ch = conv_saved.shape[1]
    n_taps = conv_taps.shape[0]
    part = width // n_sp
    dma = pltpu.SemaphoreType.DMA
    V = pltpu.VMEM
    bf = jnp.bfloat16
    vm = pl.BlockSpec(memory_space=pltpu.VMEM)
    hb = pl.BlockSpec(memory_space=pl.ANY)
    grad_value, grad_gate, grad_weight, grad_taps = pl.pallas_call(
        functools.partial(kernel, n_sp, n_tp, fold),
        out_shape=(
            jax.ShapeDtypeStruct((ch, rows), bf),
            jax.ShapeDtypeStruct((ch, rows), bf),
            jax.ShapeDtypeStruct((ch, part), f32),
            jax.ShapeDtypeStruct((n_taps, ch), f32),
        ),
        in_specs=[hb, hb, vm, vm, vm, hb, hb],
        out_specs=[vm] * 4,
        scratch_shapes=[
            V((ch, rows), bf), V((ch, rows), bf), V((ch, width), bf), V((width, rows), bf), dma((4,)),
            V((ch, 128), f32), V((rows, ch), f32), V((rows, ch), f32),
            V((ch, rows), bf), V((ch, rows), f32), V((rows + 32, ch), f32), V((8, rows + 32, ch), f32),
            V((8, rows), f32), V((8, rows), f32),
            V((n_sp, ch, part), f32), V((n_z, ch, part), f32), V((n_z, ch, part), f32),
            V((n_z, ch, part), f32),
            V((8, rows), f32), V((n_tp - 1, 8, rows), f32), V((8, rows), f32), V((n_tp - 1, 8, rows), f32),
            V((n_taps, 8, ch), f32), V((32, ch), f32), V((32, ch), f32), V((n_z - 1, 32, ch), f32),
            V((32, ch), f32), V((n_taps, 8, ch), f32),
            dma((n_tp - 1,)), dma((n_tp - 1,)), dma((n_tp - 1,)), dma((n_tp - 1,)),
            dma((n_z,)), dma((n_z,)), dma((n_z,)), dma((n_z,)), dma((n_z,)), dma((n_z,)),
            dma, dma, dma((n_z - 1,)), dma((n_z - 1,)), dma, dma,
        ],
        compiler_params=pltpu.CompilerParams(
            collective_id=0, has_side_effects=True, vmem_limit_bytes=60 * 1024 * 1024
        ),
    )(
        proj_value.T, proj_gate.T, conv_saved.T, conv_taps, norm_gain.reshape(1, ch), out_weight,
        cotangent.T,
    )
    return grad_value.T, grad_gate.T, grad_weight, grad_taps


def passed_along(block, axis, distance):
    devices = range(lax.axis_size(axis))
    route = [(i - distance, i) for i in devices if i - distance in devices]
    return lax.ppermute(block, axis, route)


def local(proj_value, proj_gate, conv_saved, conv_taps, norm_gain, out_weight, cotangent):
    model_width = cotangent.shape[1]
    tok_rows = cotangent.shape[0]
    tap_count = conv_taps.shape[0]
    overhang = tap_count - 1
    grad_scale = 1.0 / math.sqrt(tok_rows * lax.axis_size("sp"))
    conv_f = conv_saved.astype(jnp.float32)
    totals = lax.psum((jnp.sum(conv_f, axis=1), jnp.sum(conv_f * conv_f, axis=1)), "tp")
    row_mean = totals[0] / model_width
    row_var = totals[1] / model_width - row_mean * row_mean
    inv_std = lax.rsqrt(row_var + norm_eps)
    centered = (conv_f - row_mean[:, None]) * inv_std[:, None]
    gain_f = norm_gain.astype(jnp.float32)
    normed = centered * gain_f
    gate_norm = jax.nn.sigmoid(normed)
    activated = (normed * gate_norm).astype(jnp.bfloat16)
    contract_rows = (((0,), (0,)), ((), ()))
    whole_term = lax.dot_general(
        cotangent, activated, contract_rows, preferred_element_type=jnp.float32
    )
    shard_grad = lax.psum_scatter(whole_term, "sp", scatter_dimension=0, tiled=True)
    grad_out_weight = shard_grad.T * grad_scale
    d_act = lax.dot_general(
        cotangent, out_weight, (((1,), (1,)), ((), ())), preferred_element_type=jnp.float32
    )
    d_hat = d_act * gate_norm * (1.0 + normed * (1.0 - gate_norm)) * gain_f
    moments = lax.psum((jnp.sum(d_hat, axis=1), jnp.sum(d_hat * centered, axis=1)), "tp")
    first = moments[0] / model_width
    second = moments[1] / model_width
    d_conv = inv_std[:, None] * (d_hat - first[:, None] - centered * second[:, None])
    ahead = passed_along(d_conv[:overhang], "sp", -1)
    extended = jnp.concatenate([d_conv, ahead], axis=0)
    gate_proj = jax.nn.sigmoid(proj_gate.astype(jnp.float32))
    gated = proj_value.astype(jnp.float32) * gate_proj
    taps_f = conv_taps.astype(jnp.float32)
    d_glu = jnp.zeros_like(d_conv)
    tap_rows = []
    for offset in range(tap_count):
        shifted = extended[overhang - offset : overhang - offset + tok_rows]
        d_glu = d_glu + taps_f[offset] * shifted
        tap_rows.append(jnp.sum(gated * shifted, axis=0))
    grad_taps = lax.psum(jnp.stack(tap_rows), "sp") * grad_scale
    grad_value = (d_glu * gate_proj).astype(jnp.bfloat16)
    grad_gate = (d_glu * gated * (1.0 - gate_proj)).astype(jnp.bfloat16)
    return (grad_value, grad_gate, grad_out_weight, grad_taps)


def solution(mesh):
    in_specs = (
        P("sp", "tp"),
        P("sp", "tp"),
        P("sp", "tp"),
        P(None, "tp"),
        P("tp"),
        P("tp", None),
        P("sp", None),
    )
    out_specs = (P("sp", "tp"), P("sp", "tp"), P("tp", "sp"), P(None, "tp"))
    n_sp, n_tp = mesh.shape["sp"], mesh.shape["tp"]

    def step(*args):
        rows, width = args[6].shape
        ch, n_taps = args[2].shape[1], args[3].shape[0]
        small = n_sp % 2 == 0 and 4 <= n_sp <= 8 and width % n_sp == 0 and n_tp > 1
        if small and rows % 128 == 0 and rows >= 128 and ch % 8 == 0 and 24 < n_taps <= 31:
            return fused(n_sp, n_tp, *args)
        return local(*args)

    return jax.shard_map(step, mesh=mesh, in_specs=in_specs, out_specs=out_specs, check_vma=False)
```

```python
import functools
import math

import jax
import jax.numpy as jnp
from jax import lax
from jax.experimental import pallas as pl
from jax.experimental.pallas import tpu as pltpu
from jax.sharding import PartitionSpec as P

norm_eps = 1e-05
MESH = pl.DeviceIdType.MESH
f32 = jnp.float32


def line_order(length):
    rows = []
    for place in range(length):
        side = 1 if 2 * place >= length else -1
        rows.append(sorted(range(length), key=lambda d: (-abs(d - place), -side * (d - place))))
    return rows


def low_rows(ch):
    return max(ch // 7 // 8 * 8, 8)


def lookup(table, place):
    value = table[0]
    for i in range(1, len(table)):
        value = jnp.where(place == i, table[i], value)
    return value


def finish(v_in, g_in, w_in, t_in, v_out, g_out, w_out, t_out, v_b, g_b, w_b, t_b, ss):
    trips = [(v_in, v_b, v_out), (g_in, g_b, g_out), (w_in, w_b, w_out), (t_in, t_b, t_out)]
    inward = [pltpu.make_async_copy(a, b, ss.at[i]) for i, (a, b, _) in enumerate(trips)]
    outward = [pltpu.make_async_copy(b, c, ss.at[4 + i]) for i, (_, b, c) in enumerate(trips)]
    for c in inward:
        c.start()
    for a, b in zip(inward, outward):
        a.wait()
        b.start()
    for b in outward:
        b.wait()


def kernel(
    n_sp, n_tp, fold, pv_h, pg_h, conv, taps, gain, weight_h, cot_h,
    out_v, out_g, out_w, out_t,
    pv, pg, weight, cot, in_sems, gain_c, gated_s, d_glu_s, act_t, d_act, ext, shifted, cols, cols2, term, got_y, got_r, got_l, low_r, low_l, low_y,
    stat, stat_in, mom, mom_in, grad_acc, g_own, g_mid, g_in, g_yin, taps_b,
    stat_ss, stat_rs, mom_ss, mom_rs, y_ss, y_rs, r_ss, r_rs, l_ss, l_rs,
    lr_ss, lr_rs, ll_ss, ll_rs, ly_ss, ly_rs,
    halo_ss, halo_rs, gz_ss, gz_rs, gy_ss, gy_rs,
):
    s = lax.axis_index("sp")
    t = lax.axis_index("tp")
    n_z = n_sp // fold
    z = s // fold
    y = s % fold
    other_y = 1 - y
    width, rows = cot.shape
    ch = conv.shape[0]
    part = out_w.shape[1]
    n_taps = taps.shape[0]
    scale = 1.0 / math.sqrt(rows * n_sp)
    blk = 128
    n_blk = rows // blk
    low = low_rows(ch)
    top = ch - low

    loads = [
        pltpu.make_async_copy(a, b, in_sems.at[i])
        for i, (a, b) in enumerate([(cot_h, cot), (weight_h, weight), (pv_h, pv), (pg_h, pg)])
    ]
    for c in loads:
        c.start()

    barrier = pltpu.get_barrier_semaphore()
    for i in range(1, n_sp):
        pl.semaphore_signal(barrier, inc=1, device_id=(lax.rem(s + i, n_sp), t), device_id_type=MESH)
    for i in range(1, n_tp):
        pl.semaphore_signal(barrier, inc=1, device_id=(s, lax.rem(t + i, n_tp)), device_id_type=MESH)

    row8b = lax.broadcasted_iota(jnp.int32, (8, blk), 0)

    @pl.loop(0, n_blk)
    def _(i):
        at = pl.ds(pl.multiple_of(i * blk, blk), blk)
        c = conv[:, at].astype(f32)
        stat[:, at] = jnp.where(
            row8b == 0, jnp.sum(c, axis=0, keepdims=True), jnp.sum(c * c, axis=0, keepdims=True)
        )

    pl.semaphore_wait(barrier, n_sp - 1 + n_tp - 1)

    def tp_copies(src, dst, ss, rs):
        return [
            pltpu.make_async_remote_copy(
                src_ref=src, dst_ref=dst.at[i - 1], send_sem=ss.at[i - 1], recv_sem=rs.at[i - 1],
                device_id=(s, lax.rem(t + i, n_tp)), device_id_type=MESH,
            )
            for i in range(1, n_tp)
        ]

    stat_copies = tp_copies(stat, stat_in, stat_ss, stat_rs)
    for c in stat_copies:
        c.start()

    gain_c[...] = jnp.broadcast_to(gain[...].astype(f32).reshape(1, ch), (128, ch)).T
    loads[0].wait()
    loads[1].wait()
    wide_blk = 256 if rows % 256 == 0 else 128

    @pl.loop(0, rows // wide_blk)
    def _(i):
        at = pl.ds(pl.multiple_of(i * wide_blk, wide_blk), wide_blk)
        d_act[:, at] = jnp.dot(weight[...], cot[:, at], preferred_element_type=f32)

    for c in stat_copies:
        c.wait()
    total = stat[...]
    for i in range(n_tp - 1):
        total = total + stat_in[i]
    mean = total[0:1] / width
    inv = lax.rsqrt(total[1:2] / width - mean * mean + norm_eps)
    row8 = lax.broadcasted_iota(jnp.int32, (8, rows), 0)
    cols[...] = jnp.where(row8 == 0, mean, inv)

    @pl.loop(0, n_blk)
    def _(i):
        at = pl.ds(pl.multiple_of(i * blk, blk), blk)
        c = conv[:, at].astype(f32)
        normed = (c - cols[0:1, at]) * cols[1:2, at] * gain_c[...]
        act_t[:, at] = (normed * jax.nn.sigmoid(normed)).astype(jnp.bfloat16)

    for j in range(n_sp):
        term[j] = lax.dot_general(
            act_t[...], cot[j * part:(j + 1) * part, :], (((1,), (1,)), ((), ())),
            preferred_element_type=f32,
        )

    orders = line_order(n_z)
    dest = [lookup([orders[i][k] for i in range(n_z)], z) for k in range(n_z)]

    def y_copy(k):
        return pltpu.make_async_remote_copy(
            src_ref=term.at[dest[k] * fold + other_y, pl.ds(0, top), :], dst_ref=got_y.at[dest[k]],
            send_sem=y_ss.at[dest[k]], recv_sem=y_rs.at[dest[k]],
            device_id=(z * fold + other_y, t), device_id_type=MESH,
        )

    y_copies = [y_copy(k) for k in range(n_z)]

    def line_copy(d, up):
        buf, ss, rs = (got_r, r_ss, r_rs) if up else (got_l, l_ss, l_rs)
        to = z + 1 if up else z - 1
        to = jnp.clip(to, 0, n_z - 1)
        return pltpu.make_async_remote_copy(
            src_ref=term.at[d * fold + y, pl.ds(0, top), :], dst_ref=buf.at[d], send_sem=ss.at[d], recv_sem=rs.at[d],
            device_id=(to * fold + y, t), device_id_type=MESH,
        )

    def add_into(d, buf):
        own = d * fold + y
        step = max(c for c in range(8, 65, 8) if top % c == 0)

        @pl.loop(0, top // step)
        def _(i):
            at = pl.ds(pl.multiple_of(i * step, 8), step)
            term[own, at, :] = term[own, at, :] + buf[d, at, :]

    def hop(k):
        d = dest[k]
        y_copies[k].wait_recv()
        add_into(d, got_y)

        @pl.when(d > z)
        def _():
            @pl.when(z > 0)
            def _():
                line_copy(d, True).wait_recv()
                add_into(d, got_r)

            line_copy(d, True).start()

        @pl.when(d < z)
        def _():
            @pl.when(z < n_z - 1)
            def _():
                line_copy(d, False).wait_recv()
                add_into(d, got_l)

            line_copy(d, False).start()

    def low_copy(d, up):
        buf, ss, rs = (low_r, lr_ss, lr_rs) if up else (low_l, ll_ss, ll_rs)
        to = jnp.clip(z + 1 if up else z - 1, 0, n_z - 1)
        return pltpu.make_async_remote_copy(
            src_ref=term.at[pl.ds(d * fold, fold), pl.ds(top, low), :], dst_ref=buf.at[d],
            send_sem=ss.at[d], recv_sem=rs.at[d], device_id=(to * fold + y, t), device_id_type=MESH,
        )

    def low_take(d, up):
        low_copy(d, up).wait_recv()
        buf = low_r if up else low_l
        at = pl.ds(d * fold, fold)
        term[at, pl.ds(top, low), :] = term[at, pl.ds(top, low), :] + buf[d]

    def low_hop(k):
        d = dest[k]

        @pl.when(d > z)
        def _():
            @pl.when(z > 0)
            def _():
                low_take(d, True)

            low_copy(d, True).start()

        @pl.when(d < z)
        def _():
            @pl.when(z < n_z - 1)
            def _():
                low_take(d, False)

            low_copy(d, False).start()

    low_swap = pltpu.make_async_remote_copy(
        src_ref=term.at[z * fold + other_y, pl.ds(top, low), :], dst_ref=low_y,
        send_sem=ly_ss, recv_sem=ly_rs, device_id=(z * fold + other_y, t), device_id_type=MESH,
    )

    def low_end():
        @pl.when(z > 0)
        def _():
            low_take(z, True)

        @pl.when(z < n_z - 1)
        def _():
            low_take(z, False)

        low_swap.start()

    y_copies[0].start()
    y_copies[1].start()

    @pl.when(jnp.logical_or(z == 0, z == n_z - 1))
    def _():
        for k in range(n_z - 1):
            low_hop(k)

    @pl.loop(0, n_blk)
    def _(i):
        at = pl.ds(pl.multiple_of(i * blk, blk), blk)
        c = conv[:, at].astype(f32)
        centered = (c - cols[0:1, at]) * cols[1:2, at]
        normed = centered * gain_c[...]
        gate = jax.nn.sigmoid(normed)
        d_hat = d_act[:, at] * gate * (1.0 + normed * (1.0 - gate)) * gain_c[...]
        d_act[:, at] = d_hat
        mom[:, at] = jnp.where(
            row8b == 0, jnp.sum(d_hat, axis=0, keepdims=True),
            jnp.sum(d_hat * centered, axis=0, keepdims=True),
        )

    mid = jnp.logical_and(z > 0, z < n_z - 1)
    mom_copies = tp_copies(mom, mom_in, mom_ss, mom_rs)
    for c in mom_copies:
        c.start()
    for k in range(n_taps):
        taps_b[k] = jnp.broadcast_to(taps[k:k + 1, :].astype(f32), (8, ch))
    grad_acc[...] = jnp.zeros_like(grad_acc)
    loads[2].wait()
    loads[3].wait()

    @pl.loop(0, n_blk)
    def _(i):
        at = pl.ds(pl.multiple_of(i * blk, blk), blk)
        gated_s[at, :] = (pv[:, at].astype(f32) * jax.nn.sigmoid(pg[:, at].astype(f32))).T

    for c in mom_copies:
        c.wait()
    total = mom[...]
    for i in range(n_tp - 1):
        total = total + mom_in[i]
    cols2[...] = total / width

    @pl.loop(0, n_blk)
    def _(i):
        at = pl.ds(pl.multiple_of(i * blk, blk), blk)
        c = conv[:, at].astype(f32)
        inv_std = cols[1:2, at]
        centered = (c - cols[0:1, at]) * inv_std
        ext[at, :] = (inv_std * (d_act[:, at] - cols2[0:1, at] - centered * cols2[1:2, at])).T

    reach = 32
    back = jnp.maximum(s - 1, 0)
    halo = pltpu.make_async_remote_copy(
        src_ref=ext.at[pl.ds(0, reach), :], dst_ref=ext.at[pl.ds(rows, reach), :],
        send_sem=halo_ss, recv_sem=halo_rs, device_id=(back, t), device_id_type=MESH,
    )

    @pl.when(s > 0)
    def _():
        halo.start()

    for k in range(2, n_z):
        y_copies[k].start()

    def shift_block(i):
        start = pl.multiple_of(i * reach, reach)
        win = ext[pl.ds(start, reach + 8), :]
        for o in range(8):
            shifted[o, pl.ds(start, reach), :] = win[o:o + reach]

    lanes = [(lo, min(128, ch - lo)) for lo in range(0, ch, 128)]

    def conv_blocks(first, last):
        for lo, wide in lanes:
            ln = slice(lo, lo + wide)

            def body(i, accs):
                start = pl.multiple_of(i * reach, reach)
                at = pl.ds(start, reach)
                gated = gated_s[at, ln]
                d_glu = jnp.zeros((reach, wide), f32)
                out = []
                for o in range(n_taps):
                    x = shifted[o % 8, pl.ds(pl.multiple_of(start + 8 * (o // 8), 8), reach), ln]
                    tap = taps_b[n_taps - 1 - o, :, ln]
                    d_glu = d_glu + jnp.concatenate([tap] * (reach // 8), axis=0) * x
                    prod = gated * x
                    acc = accs[o]
                    for q in range(reach // 8):
                        acc = acc + prod[8 * q:8 * q + 8]
                    out.append(acc)
                d_glu_s[at, ln] = d_glu
                return tuple(out)

            accs = tuple(grad_acc[n_taps - 1 - o, :, ln] for o in range(n_taps))
            accs = lax.fori_loop(first, last, body, accs)
            for o in range(n_taps):
                grad_acc[n_taps - 1 - o, :, ln] = accs[o]

    n_row = rows // reach

    @pl.when(mid)
    def _():
        for k in range(n_z - 1):
            low_hop(k)


    @pl.loop(0, n_row - 1)
    def _(i):
        shift_block(i)

    hop(0)
    low_end()
    half = (n_row - 2) // 2
    conv_blocks(0, half)
    hop(1)
    conv_blocks(half, n_row - 2)

    @pl.when(s < n_sp - 1)
    def _():
        halo.wait_recv()

    @pl.when(s == n_sp - 1)
    def _():
        ext[pl.ds(rows, reach), :] = jnp.zeros((reach, ch), f32)

    shift_block(n_row - 1)
    win = ext[pl.ds(rows, reach), :]
    for o in range(8):
        shifted[o, pl.ds(rows, reach - 8), :] = win[o:o + reach - 8]
    conv_blocks(n_row - 2, n_row)

    for k in range(n_taps):
        g_own[k:k + 1, :] = jnp.sum(grad_acc[k], axis=0, keepdims=True)
    for k in range(n_taps, g_own.shape[0]):
        g_own[k:k + 1, :] = jnp.zeros((1, ch), f32)
    gz_copies = [
        pltpu.make_async_remote_copy(
            src_ref=g_own, dst_ref=g_in.at[i - 1], send_sem=gz_ss.at[i - 1], recv_sem=gz_rs.at[i - 1],
            device_id=(lax.rem(z + i, n_z) * fold + y, t), device_id_type=MESH,
        )
        for i in range(1, n_z)
    ]
    for c in gz_copies:
        c.start()
    for k in range(2, n_z - 1):
        hop(k)

    @pl.loop(0, n_blk)
    def _(i):
        at = pl.ds(pl.multiple_of(i * blk, blk), blk)
        gate = jax.nn.sigmoid(pg[:, at].astype(f32))
        d_glu = d_glu_s[at, :].T
        out_v[:, at] = (d_glu * gate).astype(jnp.bfloat16)
        out_g[:, at] = (d_glu * (pv[:, at].astype(f32) * gate) * (1.0 - gate)).astype(jnp.bfloat16)

    for c in gz_copies:
        c.wait()
    total = g_own[...]
    for i in range(n_z - 1):
        total = total + g_in[i]
    g_mid[...] = total
    gy = pltpu.make_async_remote_copy(
        src_ref=g_mid, dst_ref=g_yin, send_sem=gy_ss, recv_sem=gy_rs,
        device_id=(z * fold + other_y, t), device_id_type=MESH,
    )
    gy.start()
    y_copies[n_z - 1].wait_recv()
    add_into(z, got_y)

    @pl.when(z > 0)
    def _():
        line_copy(z, True).wait_recv()
        add_into(z, got_r)

    @pl.when(z < n_z - 1)
    def _():
        line_copy(z, False).wait_recv()
        add_into(z, got_l)

    low_swap.wait()
    own = z * fold + y
    out_w[:top, :] = term[own, :top, :] * scale
    out_w[top:, :] = (term[own, top:, :] + low_y[...]) * scale
    gy.wait()
    out_t[...] = ((g_mid[...] + g_yin[...]) * scale)[:n_taps]
    for k in range(n_z):
        y_copies[k].wait_send()

    @pl.when(s > 0)
    def _():
        halo.wait_send()

    for k in range(n_z - 1):
        d = dest[k]

        @pl.when(d > z)
        def _():
            line_copy(d, True).wait_send()
            low_copy(d, True).wait_send()

        @pl.when(d < z)
        def _():
            line_copy(d, False).wait_send()
            low_copy(d, False).wait_send()


def fused(n_sp, n_tp, proj_value, proj_gate, conv_saved, conv_taps, norm_gain, out_weight, cotangent):
    fold = 2
    n_z = n_sp // fold
    rows, width = cotangent.shape
    ch = conv_saved.shape[1]
    n_taps = conv_taps.shape[0]
    part = width // n_sp
    low = low_rows(ch)
    top = ch - low
    dma = pltpu.SemaphoreType.DMA
    V = pltpu.VMEM
    bf = jnp.bfloat16
    vm = pl.BlockSpec(memory_space=pltpu.VMEM)
    hb = pl.BlockSpec(memory_space=pl.ANY)
    grad_value, grad_gate, grad_weight, grad_taps = pl.pallas_call(
        functools.partial(kernel, n_sp, n_tp, fold),
        out_shape=(
            jax.ShapeDtypeStruct((ch, rows), bf),
            jax.ShapeDtypeStruct((ch, rows), bf),
            jax.ShapeDtypeStruct((ch, part), f32),
            jax.ShapeDtypeStruct((n_taps, ch), f32),
        ),
        in_specs=[hb, hb, vm, vm, vm, hb, hb],
        out_specs=[vm] * 4,
        scratch_shapes=[
            V((ch, rows), bf), V((ch, rows), bf), V((ch, width), bf), V((width, rows), bf), dma((4,)),
            V((ch, 128), f32), V((rows, ch), f32), V((rows, ch), f32),
            V((ch, rows), bf), V((ch, rows), f32), V((rows + 32, ch), f32), V((8, rows + 32, ch), f32),
            V((8, rows), f32), V((8, rows), f32),
            V((n_sp, ch, part), f32), V((n_z, top, part), f32), V((n_z, top, part), f32),
            V((n_z, top, part), f32),
            V((n_z, fold, low, part), f32), V((n_z, fold, low, part), f32), V((low, part), f32),
            V((8, rows), f32), V((n_tp - 1, 8, rows), f32), V((8, rows), f32), V((n_tp - 1, 8, rows), f32),
            V((n_taps, 8, ch), f32), V((32, ch), f32), V((32, ch), f32), V((n_z - 1, 32, ch), f32),
            V((32, ch), f32), V((n_taps, 8, ch), f32),
            dma((n_tp - 1,)), dma((n_tp - 1,)), dma((n_tp - 1,)), dma((n_tp - 1,)),
            dma((n_z,)), dma((n_z,)), dma((n_z,)), dma((n_z,)), dma((n_z,)), dma((n_z,)),
            dma((n_z,)), dma((n_z,)), dma((n_z,)), dma((n_z,)), dma, dma,
            dma, dma, dma((n_z - 1,)), dma((n_z - 1,)), dma, dma,
        ],
        compiler_params=pltpu.CompilerParams(
            collective_id=0, has_side_effects=True, vmem_limit_bytes=60 * 1024 * 1024
        ),
    )(
        proj_value.T, proj_gate.T, conv_saved.T, conv_taps, norm_gain, out_weight,
        cotangent.T,
    )
    results = (grad_value, grad_gate, grad_weight, grad_taps)
    grad_value, grad_gate, grad_weight, grad_taps = pl.pallas_call(
        finish,
        out_shape=tuple(jax.ShapeDtypeStruct(r.shape, r.dtype) for r in results),
        in_specs=[hb] * 4,
        out_specs=[hb] * 4,
        scratch_shapes=[V(r.shape, r.dtype) for r in results] + [dma((8,))],
        compiler_params=pltpu.CompilerParams(vmem_limit_bytes=60 * 1024 * 1024),
    )(*results)
    return grad_value.T, grad_gate.T, grad_weight, grad_taps


def passed_along(block, axis, distance):
    devices = range(lax.axis_size(axis))
    route = [(i - distance, i) for i in devices if i - distance in devices]
    return lax.ppermute(block, axis, route)


def local(proj_value, proj_gate, conv_saved, conv_taps, norm_gain, out_weight, cotangent):
    model_width = cotangent.shape[1]
    tok_rows = cotangent.shape[0]
    tap_count = conv_taps.shape[0]
    overhang = tap_count - 1
    grad_scale = 1.0 / math.sqrt(tok_rows * lax.axis_size("sp"))
    conv_f = conv_saved.astype(jnp.float32)
    totals = lax.psum((jnp.sum(conv_f, axis=1), jnp.sum(conv_f * conv_f, axis=1)), "tp")
    row_mean = totals[0] / model_width
    row_var = totals[1] / model_width - row_mean * row_mean
    inv_std = lax.rsqrt(row_var + norm_eps)
    centered = (conv_f - row_mean[:, None]) * inv_std[:, None]
    gain_f = norm_gain.astype(jnp.float32)
    normed = centered * gain_f
    gate_norm = jax.nn.sigmoid(normed)
    activated = (normed * gate_norm).astype(jnp.bfloat16)
    contract_rows = (((0,), (0,)), ((), ()))
    whole_term = lax.dot_general(
        cotangent, activated, contract_rows, preferred_element_type=jnp.float32
    )
    shard_grad = lax.psum_scatter(whole_term, "sp", scatter_dimension=0, tiled=True)
    grad_out_weight = shard_grad.T * grad_scale
    d_act = lax.dot_general(
        cotangent, out_weight, (((1,), (1,)), ((), ())), preferred_element_type=jnp.float32
    )
    d_hat = d_act * gate_norm * (1.0 + normed * (1.0 - gate_norm)) * gain_f
    moments = lax.psum((jnp.sum(d_hat, axis=1), jnp.sum(d_hat * centered, axis=1)), "tp")
    first = moments[0] / model_width
    second = moments[1] / model_width
    d_conv = inv_std[:, None] * (d_hat - first[:, None] - centered * second[:, None])
    ahead = passed_along(d_conv[:overhang], "sp", -1)
    extended = jnp.concatenate([d_conv, ahead], axis=0)
    gate_proj = jax.nn.sigmoid(proj_gate.astype(jnp.float32))
    gated = proj_value.astype(jnp.float32) * gate_proj
    taps_f = conv_taps.astype(jnp.float32)
    d_glu = jnp.zeros_like(d_conv)
    tap_rows = []
    for offset in range(tap_count):
        shifted = extended[overhang - offset : overhang - offset + tok_rows]
        d_glu = d_glu + taps_f[offset] * shifted
        tap_rows.append(jnp.sum(gated * shifted, axis=0))
    grad_taps = lax.psum(jnp.stack(tap_rows), "sp") * grad_scale
    grad_value = (d_glu * gate_proj).astype(jnp.bfloat16)
    grad_gate = (d_glu * gated * (1.0 - gate_proj)).astype(jnp.bfloat16)
    return (grad_value, grad_gate, grad_out_weight, grad_taps)


def solution(mesh):
    in_specs = (
        P("sp", "tp"),
        P("sp", "tp"),
        P("sp", "tp"),
        P(None, "tp"),
        P("tp"),
        P("tp", None),
        P("sp", None),
    )
    out_specs = (P("sp", "tp"), P("sp", "tp"), P("tp", "sp"), P(None, "tp"))
    n_sp, n_tp = mesh.shape["sp"], mesh.shape["tp"]

    def step(*args):
        rows, width = args[6].shape
        ch, n_taps = args[2].shape[1], args[3].shape[0]
        small = n_sp % 2 == 0 and 4 <= n_sp <= 8 and width % n_sp == 0 and n_tp > 1
        if small and rows % 128 == 0 and rows >= 128 and ch % 8 == 0 and 24 < n_taps <= 31:
            return fused(n_sp, n_tp, *args)
        return local(*args)

    return jax.shard_map(step, mesh=mesh, in_specs=in_specs, out_specs=out_specs, check_vma=False)
```

```python
import functools
import math

import jax
import jax.numpy as jnp
from jax import lax
from jax.experimental import pallas as pl
from jax.experimental.pallas import tpu as pltpu
from jax.sharding import PartitionSpec as P

norm_eps = 1e-05
MESH = pl.DeviceIdType.MESH
f32 = jnp.float32


def line_order(length):
    rows = []
    for place in range(length):
        side = 1 if 2 * place >= length else -1
        rows.append(sorted(range(length), key=lambda d: (-abs(d - place), -side * (d - place))))
    return rows


def low_rows(ch):
    return max(ch // 7 // 8 * 8, 8)


def lookup(table, place):
    value = table[0]
    for i in range(1, len(table)):
        value = jnp.where(place == i, table[i], value)
    return value


def finish(v_in, g_in, w_in, t_in, v_out, g_out, w_out, t_out, v_b, g_b, w_b, t_b, ss):
    trips = [(v_in, v_b, v_out), (g_in, g_b, g_out), (w_in, w_b, w_out), (t_in, t_b, t_out)]
    inward = [pltpu.make_async_copy(a, b, ss.at[i]) for i, (a, b, _) in enumerate(trips)]
    outward = [pltpu.make_async_copy(b, c, ss.at[4 + i]) for i, (_, b, c) in enumerate(trips)]
    for c in inward:
        c.start()
    for a, b in zip(inward, outward):
        a.wait()
        b.start()
    for b in outward:
        b.wait()


def kernel(
    n_sp, n_tp, fold, pv_h, pg_h, conv, taps, gain, weight_h, cot_h,
    out_v, out_g, out_w, out_t,
    pv, pg, weight, cot, in_sems, gain_c, gated_s, d_glu_s, act_t, d_act, ext, shifted, cols, cols2, term, got_y, got_r, got_l, low_r, low_l, low_y,
    stat, stat_in, mom, mom_in, grad_acc, g_own, g_mid, g_in, g_yin, taps_b,
    stat_ss, stat_rs, mom_ss, mom_rs, y_ss, y_rs, r_ss, r_rs, l_ss, l_rs,
    lr_ss, lr_rs, ll_ss, ll_rs, ly_ss, ly_rs,
    halo_ss, halo_rs, gz_ss, gz_rs, gy_ss, gy_rs,
):
    s = lax.axis_index("sp")
    t = lax.axis_index("tp")
    n_z = n_sp // fold
    z = s // fold
    y = s % fold
    other_y = 1 - y
    width, rows = cot.shape
    ch = conv.shape[0]
    part = out_w.shape[1]
    n_taps = taps.shape[0]
    scale = 1.0 / math.sqrt(rows * n_sp)
    blk = 128
    n_blk = rows // blk
    low = low_rows(ch)
    top = ch - low

    loads = [
        pltpu.make_async_copy(a, b, in_sems.at[i])
        for i, (a, b) in enumerate([(cot_h, cot), (weight_h, weight), (pv_h, pv), (pg_h, pg)])
    ]
    for c in loads:
        c.start()

    barrier = pltpu.get_barrier_semaphore()
    for i in range(1, n_sp):
        pl.semaphore_signal(barrier, inc=1, device_id=(lax.rem(s + i, n_sp), t), device_id_type=MESH)
    for i in range(1, n_tp):
        pl.semaphore_signal(barrier, inc=1, device_id=(s, lax.rem(t + i, n_tp)), device_id_type=MESH)

    row8b = lax.broadcasted_iota(jnp.int32, (8, blk), 0)

    @pl.loop(0, n_blk)
    def _(i):
        at = pl.ds(pl.multiple_of(i * blk, blk), blk)
        c = conv[:, at].astype(f32)
        stat[:, at] = jnp.where(
            row8b == 0, jnp.sum(c, axis=0, keepdims=True), jnp.sum(c * c, axis=0, keepdims=True)
        )

    pl.semaphore_wait(barrier, n_sp - 1 + n_tp - 1)

    def tp_copies(src, dst, ss, rs):
        return [
            pltpu.make_async_remote_copy(
                src_ref=src, dst_ref=dst.at[i - 1], send_sem=ss.at[i - 1], recv_sem=rs.at[i - 1],
                device_id=(s, lax.rem(t + i, n_tp)), device_id_type=MESH,
            )
            for i in range(1, n_tp)
        ]

    stat_copies = tp_copies(stat, stat_in, stat_ss, stat_rs)
    for c in stat_copies:
        c.start()

    gain_c[...] = jnp.broadcast_to(gain[...].astype(f32).reshape(1, ch), (128, ch)).T
    loads[0].wait()
    loads[1].wait()
    wide_blk = 256 if rows % 256 == 0 else 128

    @pl.loop(0, rows // wide_blk)
    def _(i):
        at = pl.ds(pl.multiple_of(i * wide_blk, wide_blk), wide_blk)
        d_act[:, at] = jnp.dot(weight[...], cot[:, at], preferred_element_type=f32)

    for c in stat_copies:
        c.wait()
    total = stat[...]
    for i in range(n_tp - 1):
        total = total + stat_in[i]
    mean = total[0:1] / width
    inv = lax.rsqrt(total[1:2] / width - mean * mean + norm_eps)
    row8 = lax.broadcasted_iota(jnp.int32, (8, rows), 0)
    cols[...] = jnp.where(row8 == 0, mean, inv)

    @pl.loop(0, n_blk)
    def _(i):
        at = pl.ds(pl.multiple_of(i * blk, blk), blk)
        c = conv[:, at].astype(f32)
        normed = (c - cols[0:1, at]) * cols[1:2, at] * gain_c[...]
        act_t[:, at] = (normed * jax.nn.sigmoid(normed)).astype(jnp.bfloat16)

    orders = line_order(n_z)
    dest = [lookup([orders[i][k] for i in range(n_z)], z) for k in range(n_z)]

    cut = top // 2 // 8 * 8
    halves = [(0, cut), (cut, top - cut)]

    def y_copy(k, h):
        at = pl.ds(*halves[h])
        sem = dest[k] * 2 + h
        return pltpu.make_async_remote_copy(
            src_ref=term.at[dest[k] * fold + other_y, at, :], dst_ref=got_y.at[dest[k], at, :],
            send_sem=y_ss.at[sem], recv_sem=y_rs.at[sem],
            device_id=(z * fold + other_y, t), device_id_type=MESH,
        )

    y_copies = [[y_copy(k, h) for h in range(2)] for k in range(n_z)]

    def make_term(j):
        term[j] = lax.dot_general(
            act_t[...], cot[j * part:(j + 1) * part, :], (((1,), (1,)), ((), ())),
            preferred_element_type=f32,
        )

    lead = dest[0] * fold + other_y
    leads = sorted({orders[i][0] * fold + o for i in range(n_z) for o in range(fold)})
    for j in leads:
        @pl.when(lead == j)
        def _():
            make_term(j)

    for h in range(2):
        y_copies[0][h].start()
    for j in range(n_sp):
        if j in leads:
            @pl.when(lead != j)
            def _():
                make_term(j)
        else:
            make_term(j)


    def line_copy(d, h, up):
        buf, ss, rs = (got_r, r_ss, r_rs) if up else (got_l, l_ss, l_rs)
        to = z + 1 if up else z - 1
        to = jnp.clip(to, 0, n_z - 1)
        return pltpu.make_async_remote_copy(
            src_ref=term.at[d * fold + y, pl.ds(*halves[h]), :], dst_ref=buf.at[d, pl.ds(*halves[h]), :],
            send_sem=ss.at[d * 2 + h], recv_sem=rs.at[d * 2 + h],
            device_id=(to * fold + y, t), device_id_type=MESH,
        )

    def add_into(d, h, buf):
        own = d * fold + y
        first, count = halves[h]
        step = max(c for c in range(8, 81, 8) if count % c == 0)

        @pl.loop(0, count // step)
        def _(i):
            at = pl.ds(pl.multiple_of(first + i * step, 8), step)
            term[own, at, :] = term[own, at, :] + buf[d, at, :]

    def hop(k, h):
        d = dest[k]
        y_copies[k][h].wait_recv()
        add_into(d, h, got_y)

        @pl.when(d > z)
        def _():
            @pl.when(z > 0)
            def _():
                line_copy(d, h, True).wait_recv()
                add_into(d, h, got_r)

            line_copy(d, h, True).start()

        @pl.when(d < z)
        def _():
            @pl.when(z < n_z - 1)
            def _():
                line_copy(d, h, False).wait_recv()
                add_into(d, h, got_l)

            line_copy(d, h, False).start()

    def low_copy(d, up):
        buf, ss, rs = (low_r, lr_ss, lr_rs) if up else (low_l, ll_ss, ll_rs)
        to = jnp.clip(z + 1 if up else z - 1, 0, n_z - 1)
        return pltpu.make_async_remote_copy(
            src_ref=term.at[pl.ds(d * fold, fold), pl.ds(top, low), :], dst_ref=buf.at[d],
            send_sem=ss.at[d], recv_sem=rs.at[d], device_id=(to * fold + y, t), device_id_type=MESH,
        )

    def low_take(d, up):
        low_copy(d, up).wait_recv()
        buf = low_r if up else low_l
        at = pl.ds(d * fold, fold)
        term[at, pl.ds(top, low), :] = term[at, pl.ds(top, low), :] + buf[d]

    def low_hop(k):
        d = dest[k]

        @pl.when(d > z)
        def _():
            @pl.when(z > 0)
            def _():
                low_take(d, True)

            low_copy(d, True).start()

        @pl.when(d < z)
        def _():
            @pl.when(z < n_z - 1)
            def _():
                low_take(d, False)

            low_copy(d, False).start()

    low_swap = pltpu.make_async_remote_copy(
        src_ref=term.at[z * fold + other_y, pl.ds(top, low), :], dst_ref=low_y,
        send_sem=ly_ss, recv_sem=ly_rs, device_id=(z * fold + other_y, t), device_id_type=MESH,
    )

    def low_end():
        @pl.when(z > 0)
        def _():
            low_take(z, True)

        @pl.when(z < n_z - 1)
        def _():
            low_take(z, False)

        low_swap.start()

    for h in range(2):
        y_copies[1][h].start()

    @pl.when(jnp.logical_or(z == 0, z == n_z - 1))
    def _():
        for k in range(n_z - 1):
            low_hop(k)

    @pl.loop(0, n_blk)
    def _(i):
        at = pl.ds(pl.multiple_of(i * blk, blk), blk)
        c = conv[:, at].astype(f32)
        centered = (c - cols[0:1, at]) * cols[1:2, at]
        normed = centered * gain_c[...]
        gate = jax.nn.sigmoid(normed)
        d_hat = d_act[:, at] * gate * (1.0 + normed * (1.0 - gate)) * gain_c[...]
        d_act[:, at] = d_hat
        mom[:, at] = jnp.where(
            row8b == 0, jnp.sum(d_hat, axis=0, keepdims=True),
            jnp.sum(d_hat * centered, axis=0, keepdims=True),
        )

    mid = jnp.logical_and(z > 0, z < n_z - 1)
    mom_copies = tp_copies(mom, mom_in, mom_ss, mom_rs)
    for c in mom_copies:
        c.start()
    for k in range(n_taps):
        taps_b[k] = jnp.broadcast_to(taps[k:k + 1, :].astype(f32), (8, ch))
    grad_acc[...] = jnp.zeros_like(grad_acc)
    loads[2].wait()
    loads[3].wait()

    @pl.loop(0, n_blk)
    def _(i):
        at = pl.ds(pl.multiple_of(i * blk, blk), blk)
        gated_s[at, :] = (pv[:, at].astype(f32) * jax.nn.sigmoid(pg[:, at].astype(f32))).T

    for c in mom_copies:
        c.wait()
    total = mom[...]
    for i in range(n_tp - 1):
        total = total + mom_in[i]
    cols2[...] = total / width

    @pl.loop(0, n_blk)
    def _(i):
        at = pl.ds(pl.multiple_of(i * blk, blk), blk)
        c = conv[:, at].astype(f32)
        inv_std = cols[1:2, at]
        centered = (c - cols[0:1, at]) * inv_std
        ext[at, :] = (inv_std * (d_act[:, at] - cols2[0:1, at] - centered * cols2[1:2, at])).T

    reach = 32
    back = jnp.maximum(s - 1, 0)
    halo = pltpu.make_async_remote_copy(
        src_ref=ext.at[pl.ds(0, reach), :], dst_ref=ext.at[pl.ds(rows, reach), :],
        send_sem=halo_ss, recv_sem=halo_rs, device_id=(back, t), device_id_type=MESH,
    )

    @pl.when(s > 0)
    def _():
        halo.start()

    for k in range(2, n_z):
        for h in range(2):
            y_copies[k][h].start()

    def shift_block(i):
        start = pl.multiple_of(i * reach, reach)
        win = ext[pl.ds(start, reach + 8), :]
        for o in range(8):
            shifted[o, pl.ds(start, reach), :] = win[o:o + reach]

    lanes = [(lo, min(128, ch - lo)) for lo in range(0, ch, 128)]

    def conv_blocks(first, last):
        for lo, wide in lanes:
            ln = slice(lo, lo + wide)

            def body(i, accs):
                start = pl.multiple_of(i * reach, reach)
                at = pl.ds(start, reach)
                gated = gated_s[at, ln]
                d_glu = jnp.zeros((reach, wide), f32)
                out = []
                for o in range(n_taps):
                    x = shifted[o % 8, pl.ds(pl.multiple_of(start + 8 * (o // 8), 8), reach), ln]
                    tap = taps_b[n_taps - 1 - o, :, ln]
                    d_glu = d_glu + jnp.concatenate([tap] * (reach // 8), axis=0) * x
                    prod = gated * x
                    acc = accs[o]
                    for q in range(reach // 8):
                        acc = acc + prod[8 * q:8 * q + 8]
                    out.append(acc)
                d_glu_s[at, ln] = d_glu
                return tuple(out)

            accs = tuple(grad_acc[n_taps - 1 - o, :, ln] for o in range(n_taps))
            accs = lax.fori_loop(first, last, body, accs)
            for o in range(n_taps):
                grad_acc[n_taps - 1 - o, :, ln] = accs[o]

    n_row = rows // reach

    @pl.when(mid)
    def _():
        for k in range(n_z - 1):
            low_hop(k)


    @pl.loop(0, n_row - 1)
    def _(i):
        shift_block(i)

    marks = [(n_row - 2) * i // 4 for i in range(5)]
    hop(0, 0)
    conv_blocks(marks[0], marks[1])
    hop(0, 1)
    low_end()
    conv_blocks(marks[1], marks[2])
    hop(1, 0)
    conv_blocks(marks[2], marks[3])
    hop(1, 1)
    conv_blocks(marks[3], marks[4])

    @pl.when(s < n_sp - 1)
    def _():
        halo.wait_recv()

    @pl.when(s == n_sp - 1)
    def _():
        ext[pl.ds(rows, reach), :] = jnp.zeros((reach, ch), f32)

    shift_block(n_row - 1)
    win = ext[pl.ds(rows, reach), :]
    for o in range(8):
        shifted[o, pl.ds(rows, reach - 8), :] = win[o:o + reach - 8]
    conv_blocks(n_row - 2, n_row)

    for k in range(n_taps):
        g_own[k:k + 1, :] = jnp.sum(grad_acc[k], axis=0, keepdims=True)
    for k in range(n_taps, g_own.shape[0]):
        g_own[k:k + 1, :] = jnp.zeros((1, ch), f32)
    gz_copies = [
        pltpu.make_async_remote_copy(
            src_ref=g_own, dst_ref=g_in.at[i - 1], send_sem=gz_ss.at[i - 1], recv_sem=gz_rs.at[i - 1],
            device_id=(lax.rem(z + i, n_z) * fold + y, t), device_id_type=MESH,
        )
        for i in range(1, n_z)
    ]
    for c in gz_copies:
        c.start()
    for k in range(2, n_z - 1):
        for h in range(2):
            hop(k, h)

    @pl.loop(0, n_blk)
    def _(i):
        at = pl.ds(pl.multiple_of(i * blk, blk), blk)
        gate = jax.nn.sigmoid(pg[:, at].astype(f32))
        d_glu = d_glu_s[at, :].T
        out_v[:, at] = (d_glu * gate).astype(jnp.bfloat16)
        out_g[:, at] = (d_glu * (pv[:, at].astype(f32) * gate) * (1.0 - gate)).astype(jnp.bfloat16)

    for c in gz_copies:
        c.wait()
    total = g_own[...]
    for i in range(n_z - 1):
        total = total + g_in[i]
    g_mid[...] = total
    gy = pltpu.make_async_remote_copy(
        src_ref=g_mid, dst_ref=g_yin, send_sem=gy_ss, recv_sem=gy_rs,
        device_id=(z * fold + other_y, t), device_id_type=MESH,
    )
    gy.start()
    for h in range(2):
        y_copies[n_z - 1][h].wait_recv()
        add_into(z, h, got_y)

        @pl.when(z > 0)
        def _():
            line_copy(z, h, True).wait_recv()
            add_into(z, h, got_r)

        @pl.when(z < n_z - 1)
        def _():
            line_copy(z, h, False).wait_recv()
            add_into(z, h, got_l)

    low_swap.wait()
    own = z * fold + y
    out_w[:top, :] = term[own, :top, :] * scale
    out_w[top:, :] = (term[own, top:, :] + low_y[...]) * scale
    gy.wait()
    out_t[...] = ((g_mid[...] + g_yin[...]) * scale)[:n_taps]
    for k in range(n_z):
        for h in range(2):
            y_copies[k][h].wait_send()

    @pl.when(s > 0)
    def _():
        halo.wait_send()

    for k in range(n_z - 1):
        d = dest[k]

        @pl.when(d > z)
        def _():
            for h in range(2):
                line_copy(d, h, True).wait_send()
            low_copy(d, True).wait_send()

        @pl.when(d < z)
        def _():
            for h in range(2):
                line_copy(d, h, False).wait_send()
            low_copy(d, False).wait_send()


def fused(n_sp, n_tp, proj_value, proj_gate, conv_saved, conv_taps, norm_gain, out_weight, cotangent):
    fold = 2
    n_z = n_sp // fold
    rows, width = cotangent.shape
    ch = conv_saved.shape[1]
    n_taps = conv_taps.shape[0]
    part = width // n_sp
    low = low_rows(ch)
    top = ch - low
    dma = pltpu.SemaphoreType.DMA
    V = pltpu.VMEM
    bf = jnp.bfloat16
    vm = pl.BlockSpec(memory_space=pltpu.VMEM)
    hb = pl.BlockSpec(memory_space=pl.ANY)
    grad_value, grad_gate, grad_weight, grad_taps = pl.pallas_call(
        functools.partial(kernel, n_sp, n_tp, fold),
        out_shape=(
            jax.ShapeDtypeStruct((ch, rows), bf),
            jax.ShapeDtypeStruct((ch, rows), bf),
            jax.ShapeDtypeStruct((ch, part), f32),
            jax.ShapeDtypeStruct((n_taps, ch), f32),
        ),
        in_specs=[hb, hb, vm, vm, vm, hb, hb],
        out_specs=[vm] * 4,
        scratch_shapes=[
            V((ch, rows), bf), V((ch, rows), bf), V((ch, width), bf), V((width, rows), bf), dma((4,)),
            V((ch, 128), f32), V((rows, ch), f32), V((rows, ch), f32),
            V((ch, rows), bf), V((ch, rows), f32), V((rows + 32, ch), f32), V((8, rows + 32, ch), f32),
            V((8, rows), f32), V((8, rows), f32),
            V((n_sp, ch, part), f32), V((n_z, top, part), f32), V((n_z, top, part), f32),
            V((n_z, top, part), f32),
            V((n_z, fold, low, part), f32), V((n_z, fold, low, part), f32), V((low, part), f32),
            V((8, rows), f32), V((n_tp - 1, 8, rows), f32), V((8, rows), f32), V((n_tp - 1, 8, rows), f32),
            V((n_taps, 8, ch), f32), V((32, ch), f32), V((32, ch), f32), V((n_z - 1, 32, ch), f32),
            V((32, ch), f32), V((n_taps, 8, ch), f32),
            dma((n_tp - 1,)), dma((n_tp - 1,)), dma((n_tp - 1,)), dma((n_tp - 1,)),
            *[dma((2 * n_z,))] * 6,
            dma((n_z,)), dma((n_z,)), dma((n_z,)), dma((n_z,)), dma, dma,
            dma, dma, dma((n_z - 1,)), dma((n_z - 1,)), dma, dma,
        ],
        compiler_params=pltpu.CompilerParams(
            collective_id=0, has_side_effects=True, vmem_limit_bytes=60 * 1024 * 1024
        ),
    )(
        proj_value.T, proj_gate.T, conv_saved.T, conv_taps, norm_gain, out_weight,
        cotangent.T,
    )
    results = (grad_value, grad_gate, grad_weight, grad_taps)
    grad_value, grad_gate, grad_weight, grad_taps = pl.pallas_call(
        finish,
        out_shape=tuple(jax.ShapeDtypeStruct(r.shape, r.dtype) for r in results),
        in_specs=[hb] * 4,
        out_specs=[hb] * 4,
        scratch_shapes=[V(r.shape, r.dtype) for r in results] + [dma((8,))],
        compiler_params=pltpu.CompilerParams(vmem_limit_bytes=60 * 1024 * 1024),
    )(*results)
    return grad_value.T, grad_gate.T, grad_weight, grad_taps


def passed_along(block, axis, distance):
    devices = range(lax.axis_size(axis))
    route = [(i - distance, i) for i in devices if i - distance in devices]
    return lax.ppermute(block, axis, route)


def local(proj_value, proj_gate, conv_saved, conv_taps, norm_gain, out_weight, cotangent):
    model_width = cotangent.shape[1]
    tok_rows = cotangent.shape[0]
    tap_count = conv_taps.shape[0]
    overhang = tap_count - 1
    grad_scale = 1.0 / math.sqrt(tok_rows * lax.axis_size("sp"))
    conv_f = conv_saved.astype(jnp.float32)
    totals = lax.psum((jnp.sum(conv_f, axis=1), jnp.sum(conv_f * conv_f, axis=1)), "tp")
    row_mean = totals[0] / model_width
    row_var = totals[1] / model_width - row_mean * row_mean
    inv_std = lax.rsqrt(row_var + norm_eps)
    centered = (conv_f - row_mean[:, None]) * inv_std[:, None]
    gain_f = norm_gain.astype(jnp.float32)
    normed = centered * gain_f
    gate_norm = jax.nn.sigmoid(normed)
    activated = (normed * gate_norm).astype(jnp.bfloat16)
    contract_rows = (((0,), (0,)), ((), ()))
    whole_term = lax.dot_general(
        cotangent, activated, contract_rows, preferred_element_type=jnp.float32
    )
    shard_grad = lax.psum_scatter(whole_term, "sp", scatter_dimension=0, tiled=True)
    grad_out_weight = shard_grad.T * grad_scale
    d_act = lax.dot_general(
        cotangent, out_weight, (((1,), (1,)), ((), ())), preferred_element_type=jnp.float32
    )
    d_hat = d_act * gate_norm * (1.0 + normed * (1.0 - gate_norm)) * gain_f
    moments = lax.psum((jnp.sum(d_hat, axis=1), jnp.sum(d_hat * centered, axis=1)), "tp")
    first = moments[0] / model_width
    second = moments[1] / model_width
    d_conv = inv_std[:, None] * (d_hat - first[:, None] - centered * second[:, None])
    ahead = passed_along(d_conv[:overhang], "sp", -1)
    extended = jnp.concatenate([d_conv, ahead], axis=0)
    gate_proj = jax.nn.sigmoid(proj_gate.astype(jnp.float32))
    gated = proj_value.astype(jnp.float32) * gate_proj
    taps_f = conv_taps.astype(jnp.float32)
    d_glu = jnp.zeros_like(d_conv)
    tap_rows = []
    for offset in range(tap_count):
        shifted = extended[overhang - offset : overhang - offset + tok_rows]
        d_glu = d_glu + taps_f[offset] * shifted
        tap_rows.append(jnp.sum(gated * shifted, axis=0))
    grad_taps = lax.psum(jnp.stack(tap_rows), "sp") * grad_scale
    grad_value = (d_glu * gate_proj).astype(jnp.bfloat16)
    grad_gate = (d_glu * gated * (1.0 - gate_proj)).astype(jnp.bfloat16)
    return (grad_value, grad_gate, grad_out_weight, grad_taps)


def solution(mesh):
    in_specs = (
        P("sp", "tp"),
        P("sp", "tp"),
        P("sp", "tp"),
        P(None, "tp"),
        P("tp"),
        P("tp", None),
        P("sp", None),
    )
    out_specs = (P("sp", "tp"), P("sp", "tp"), P("tp", "sp"), P(None, "tp"))
    n_sp, n_tp = mesh.shape["sp"], mesh.shape["tp"]

    def step(*args):
        rows, width = args[6].shape
        ch, n_taps = args[2].shape[1], args[3].shape[0]
        small = n_sp % 2 == 0 and 4 <= n_sp <= 8 and width % n_sp == 0 and n_tp > 1
        if small and rows % 128 == 0 and rows >= 128 and ch % 8 == 0 and 24 < n_taps <= 31:
            return fused(n_sp, n_tp, *args)
        return local(*args)

    return jax.shard_map(step, mesh=mesh, in_specs=in_specs, out_specs=out_specs, check_vma=False)
```

```python
import functools
import math

import jax
import jax.numpy as jnp
from jax import lax
from jax.experimental import pallas as pl
from jax.experimental.pallas import tpu as pltpu
from jax.sharding import PartitionSpec as P

norm_eps = 1e-05
MESH = pl.DeviceIdType.MESH
f32 = jnp.float32


def line_order(length):
    rows = []
    for place in range(length):
        side = 1 if 2 * place >= length else -1
        rows.append(sorted(range(length), key=lambda d: (-abs(d - place), -side * (d - place))))
    return rows


def low_rows(ch):
    return max(ch // 7 // 8 * 8, 8)


def lookup(table, place):
    value = table[0]
    for i in range(1, len(table)):
        value = jnp.where(place == i, table[i], value)
    return value


def finish(v_in, g_in, w_in, t_in, v_out, g_out, w_out, t_out, v_b, g_b, w_b, t_b, ss):
    trips = [(v_in, v_b, v_out), (g_in, g_b, g_out), (w_in, w_b, w_out), (t_in, t_b, t_out)]
    inward = [pltpu.make_async_copy(a, b, ss.at[i]) for i, (a, b, _) in enumerate(trips)]
    outward = [pltpu.make_async_copy(b, c, ss.at[4 + i]) for i, (_, b, c) in enumerate(trips)]
    for c in inward:
        c.start()
    for a, b in zip(inward, outward):
        a.wait()
        b.start()
    for b in outward:
        b.wait()


def kernel(
    n_sp, n_tp, fold, pv_h, pg_h, conv, taps, gain, weight_h, cot_h,
    out_v, out_g, out_w, out_t,
    pv, pg, weight, cot, in_sems, gain_c, gated_s, d_glu_s, act_t, d_act, ext, shifted, cols, cols2, term, got_y, got_r, got_l, low_r, low_l, low_y,
    stat, stat_in, mom, mom_in, grad_acc, g_own, g_mid, g_in, g_yin, taps_b,
    stat_ss, stat_rs, mom_ss, mom_rs, y_ss, y_rs, r_ss, r_rs, l_ss, l_rs,
    lr_ss, lr_rs, ll_ss, ll_rs, ly_ss, ly_rs,
    halo_ss, halo_rs, gz_ss, gz_rs, gy_ss, gy_rs,
):
    s = lax.axis_index("sp")
    t = lax.axis_index("tp")
    n_z = n_sp // fold
    z = s // fold
    y = s % fold
    other_y = 1 - y
    width, rows = cot.shape
    ch = conv.shape[0]
    part = out_w.shape[1]
    n_taps = taps.shape[0]
    scale = 1.0 / math.sqrt(rows * n_sp)
    blk = 128
    n_blk = rows // blk
    low = low_rows(ch)
    top = ch - low

    loads = [
        pltpu.make_async_copy(a, b, in_sems.at[i])
        for i, (a, b) in enumerate([(cot_h, cot), (weight_h, weight), (pv_h, pv), (pg_h, pg)])
    ]
    for c in loads:
        c.start()

    barrier = pltpu.get_barrier_semaphore()
    for i in range(1, n_sp):
        pl.semaphore_signal(barrier, inc=1, device_id=(lax.rem(s + i, n_sp), t), device_id_type=MESH)
    for i in range(1, n_tp):
        pl.semaphore_signal(barrier, inc=1, device_id=(s, lax.rem(t + i, n_tp)), device_id_type=MESH)

    row8b = lax.broadcasted_iota(jnp.int32, (8, blk), 0)

    @pl.loop(0, n_blk)
    def _(i):
        at = pl.ds(pl.multiple_of(i * blk, blk), blk)
        c = conv[:, at].astype(f32)
        stat[:, at] = jnp.where(
            row8b == 0, jnp.sum(c, axis=0, keepdims=True), jnp.sum(c * c, axis=0, keepdims=True)
        )

    pl.semaphore_wait(barrier, n_sp - 1 + n_tp - 1)

    def tp_copies(src, dst, ss, rs):
        return [
            pltpu.make_async_remote_copy(
                src_ref=src, dst_ref=dst.at[i - 1], send_sem=ss.at[i - 1], recv_sem=rs.at[i - 1],
                device_id=(s, lax.rem(t + i, n_tp)), device_id_type=MESH,
            )
            for i in range(1, n_tp)
        ]

    stat_copies = tp_copies(stat, stat_in, stat_ss, stat_rs)
    for c in stat_copies:
        c.start()

    gain_c[...] = jnp.broadcast_to(gain[...].astype(f32).reshape(1, ch), (128, ch)).T
    loads[0].wait()
    loads[1].wait()
    wide_blk = 256 if rows % 256 == 0 else 128

    @pl.loop(0, rows // wide_blk)
    def _(i):
        at = pl.ds(pl.multiple_of(i * wide_blk, wide_blk), wide_blk)
        d_act[:, at] = jnp.dot(weight[...], cot[:, at], preferred_element_type=f32)

    for c in stat_copies:
        c.wait()
    total = stat[...]
    for i in range(n_tp - 1):
        total = total + stat_in[i]
    mean = total[0:1] / width
    inv = lax.rsqrt(total[1:2] / width - mean * mean + norm_eps)
    row8 = lax.broadcasted_iota(jnp.int32, (8, rows), 0)
    cols[...] = jnp.where(row8 == 0, mean, inv)

    @pl.loop(0, n_blk)
    def _(i):
        at = pl.ds(pl.multiple_of(i * blk, blk), blk)
        c = conv[:, at].astype(f32)
        normed = (c - cols[0:1, at]) * cols[1:2, at] * gain_c[...]
        act_t[:, at] = (normed * jax.nn.sigmoid(normed)).astype(jnp.bfloat16)

    orders = line_order(n_z)
    dest = [lookup([orders[i][k] for i in range(n_z)], z) for k in range(n_z)]

    cut = top // 2 // 8 * 8
    halves = [(0, cut), (cut, top - cut)]

    def y_copy(k, h):
        at = pl.ds(*halves[h])
        sem = dest[k] * 2 + h
        return pltpu.make_async_remote_copy(
            src_ref=term.at[dest[k] * fold + other_y, at, :], dst_ref=got_y.at[dest[k], at, :],
            send_sem=y_ss.at[sem], recv_sem=y_rs.at[sem],
            device_id=(z * fold + other_y, t), device_id_type=MESH,
        )

    y_copies = [[y_copy(k, h) for h in range(2)] for k in range(n_z)]

    def make_term(j):
        term[j] = lax.dot_general(
            act_t[...], cot[j * part:(j + 1) * part, :], (((1,), (1,)), ((), ())),
            preferred_element_type=f32,
        )

    lead = dest[0] * fold + other_y
    leads = sorted({orders[i][0] * fold + o for i in range(n_z) for o in range(fold)})
    for j in leads:
        @pl.when(lead == j)
        def _():
            make_term(j)

    for h in range(2):
        y_copies[0][h].start()
    for j in range(n_sp):
        if j in leads:
            @pl.when(lead != j)
            def _():
                make_term(j)
        else:
            make_term(j)


    def line_copy(d, h, up):
        buf, ss, rs = (got_r, r_ss, r_rs) if up else (got_l, l_ss, l_rs)
        to = z + 1 if up else z - 1
        to = jnp.clip(to, 0, n_z - 1)
        return pltpu.make_async_remote_copy(
            src_ref=term.at[d * fold + y, pl.ds(*halves[h]), :], dst_ref=buf.at[d, pl.ds(*halves[h]), :],
            send_sem=ss.at[d * 2 + h], recv_sem=rs.at[d * 2 + h],
            device_id=(to * fold + y, t), device_id_type=MESH,
        )

    def add_into(d, h, buf):
        own = d * fold + y
        first, count = halves[h]
        step = max(c for c in range(8, 81, 8) if count % c == 0)

        @pl.loop(0, count // step)
        def _(i):
            at = pl.ds(pl.multiple_of(first + i * step, 8), step)
            term[own, at, :] = term[own, at, :] + buf[d, at, :]

    def hop(k, h):
        d = dest[k]
        y_copies[k][h].wait_recv()
        add_into(d, h, got_y)

        @pl.when(d > z)
        def _():
            @pl.when(z > 0)
            def _():
                line_copy(d, h, True).wait_recv()
                add_into(d, h, got_r)

            line_copy(d, h, True).start()

        @pl.when(d < z)
        def _():
            @pl.when(z < n_z - 1)
            def _():
                line_copy(d, h, False).wait_recv()
                add_into(d, h, got_l)

            line_copy(d, h, False).start()

    def low_copy(d, up):
        buf, ss, rs = (low_r, lr_ss, lr_rs) if up else (low_l, ll_ss, ll_rs)
        to = jnp.clip(z + 1 if up else z - 1, 0, n_z - 1)
        return pltpu.make_async_remote_copy(
            src_ref=term.at[pl.ds(d * fold, fold), pl.ds(top, low), :], dst_ref=buf.at[d],
            send_sem=ss.at[d], recv_sem=rs.at[d], device_id=(to * fold + y, t), device_id_type=MESH,
        )

    def low_take(d, up):
        low_copy(d, up).wait_recv()
        buf = low_r if up else low_l
        at = pl.ds(d * fold, fold)
        term[at, pl.ds(top, low), :] = term[at, pl.ds(top, low), :] + buf[d]

    def low_hop(k):
        d = dest[k]

        @pl.when(d > z)
        def _():
            @pl.when(z > 0)
            def _():
                low_take(d, True)

            low_copy(d, True).start()

        @pl.when(d < z)
        def _():
            @pl.when(z < n_z - 1)
            def _():
                low_take(d, False)

            low_copy(d, False).start()

    low_swap = pltpu.make_async_remote_copy(
        src_ref=term.at[z * fold + other_y, pl.ds(top, low), :], dst_ref=low_y,
        send_sem=ly_ss, recv_sem=ly_rs, device_id=(z * fold + other_y, t), device_id_type=MESH,
    )

    def low_end():
        @pl.when(z > 0)
        def _():
            low_take(z, True)

        @pl.when(z < n_z - 1)
        def _():
            low_take(z, False)

        low_swap.start()

    for h in range(2):
        y_copies[1][h].start()

    @pl.when(jnp.logical_or(z == 0, z == n_z - 1))
    def _():
        for k in range(n_z - 1):
            low_hop(k)

    @pl.loop(0, n_blk)
    def _(i):
        at = pl.ds(pl.multiple_of(i * blk, blk), blk)
        c = conv[:, at].astype(f32)
        centered = (c - cols[0:1, at]) * cols[1:2, at]
        normed = centered * gain_c[...]
        gate = jax.nn.sigmoid(normed)
        d_hat = d_act[:, at] * gate * (1.0 + normed * (1.0 - gate)) * gain_c[...]
        d_act[:, at] = d_hat
        mom[:, at] = jnp.where(
            row8b == 0, jnp.sum(d_hat, axis=0, keepdims=True),
            jnp.sum(d_hat * centered, axis=0, keepdims=True),
        )

    mid = jnp.logical_and(z > 0, z < n_z - 1)
    mom_copies = tp_copies(mom, mom_in, mom_ss, mom_rs)
    for c in mom_copies:
        c.start()
    for k in range(n_taps):
        taps_b[k] = jnp.broadcast_to(taps[k:k + 1, :].astype(f32), (8, ch))
    grad_acc[...] = jnp.zeros_like(grad_acc)
    loads[2].wait()
    loads[3].wait()

    @pl.loop(0, n_blk)
    def _(i):
        at = pl.ds(pl.multiple_of(i * blk, blk), blk)
        gated_s[at, :] = (pv[:, at].astype(f32) * jax.nn.sigmoid(pg[:, at].astype(f32))).T

    at_end = jnp.logical_or(z == 0, z == n_z - 1)

    @pl.when(at_end)
    def _():
        hop(0, 0)

    for c in mom_copies:
        c.wait()
    total = mom[...]
    for i in range(n_tp - 1):
        total = total + mom_in[i]
    cols2[...] = total / width

    @pl.loop(0, n_blk)
    def _(i):
        at = pl.ds(pl.multiple_of(i * blk, blk), blk)
        c = conv[:, at].astype(f32)
        inv_std = cols[1:2, at]
        centered = (c - cols[0:1, at]) * inv_std
        ext[at, :] = (inv_std * (d_act[:, at] - cols2[0:1, at] - centered * cols2[1:2, at])).T

    reach = 32
    back = jnp.maximum(s - 1, 0)
    halo = pltpu.make_async_remote_copy(
        src_ref=ext.at[pl.ds(0, reach), :], dst_ref=ext.at[pl.ds(rows, reach), :],
        send_sem=halo_ss, recv_sem=halo_rs, device_id=(back, t), device_id_type=MESH,
    )

    @pl.when(s > 0)
    def _():
        halo.start()

    for k in range(2, n_z):
        for h in range(2):
            y_copies[k][h].start()

    def shift_block(i):
        start = pl.multiple_of(i * reach, reach)
        win = ext[pl.ds(start, reach + 8), :]
        for o in range(8):
            shifted[o, pl.ds(start, reach), :] = win[o:o + reach]

    lanes = [(lo, min(128, ch - lo)) for lo in range(0, ch, 128)]

    def conv_blocks(first, last):
        for lo, wide in lanes:
            ln = slice(lo, lo + wide)

            def body(i, accs):
                start = pl.multiple_of(i * reach, reach)
                at = pl.ds(start, reach)
                gated = gated_s[at, ln]
                d_glu = jnp.zeros((reach, wide), f32)
                out = []
                for o in range(n_taps):
                    x = shifted[o % 8, pl.ds(pl.multiple_of(start + 8 * (o // 8), 8), reach), ln]
                    tap = taps_b[n_taps - 1 - o, :, ln]
                    d_glu = d_glu + jnp.concatenate([tap] * (reach // 8), axis=0) * x
                    prod = gated * x
                    acc = accs[o]
                    for q in range(reach // 8):
                        acc = acc + prod[8 * q:8 * q + 8]
                    out.append(acc)
                d_glu_s[at, ln] = d_glu
                return tuple(out)

            accs = tuple(grad_acc[n_taps - 1 - o, :, ln] for o in range(n_taps))
            accs = lax.fori_loop(first, last, body, accs)
            for o in range(n_taps):
                grad_acc[n_taps - 1 - o, :, ln] = accs[o]

    n_row = rows // reach

    @pl.when(mid)
    def _():
        for k in range(n_z - 1):
            low_hop(k)


    @pl.loop(0, n_row - 1)
    def _(i):
        shift_block(i)

    marks = [(n_row - 2) * i // 4 for i in range(5)]

    @pl.when(at_end)
    def _():
        hop(0, 1)

    @pl.when(mid)
    def _():
        hop(0, 0)

    conv_blocks(marks[0], marks[1])

    @pl.when(mid)
    def _():
        hop(0, 1)

    low_end()
    conv_blocks(marks[1], marks[2])
    hop(1, 0)
    conv_blocks(marks[2], marks[3])
    hop(1, 1)
    conv_blocks(marks[3], marks[4])

    @pl.when(s < n_sp - 1)
    def _():
        halo.wait_recv()

    @pl.when(s == n_sp - 1)
    def _():
        ext[pl.ds(rows, reach), :] = jnp.zeros((reach, ch), f32)

    shift_block(n_row - 1)
    win = ext[pl.ds(rows, reach), :]
    for o in range(8):
        shifted[o, pl.ds(rows, reach - 8), :] = win[o:o + reach - 8]
    conv_blocks(n_row - 2, n_row)

    for k in range(n_taps):
        g_own[k:k + 1, :] = jnp.sum(grad_acc[k], axis=0, keepdims=True)
    for k in range(n_taps, g_own.shape[0]):
        g_own[k:k + 1, :] = jnp.zeros((1, ch), f32)
    gz_copies = [
        pltpu.make_async_remote_copy(
            src_ref=g_own, dst_ref=g_in.at[i - 1], send_sem=gz_ss.at[i - 1], recv_sem=gz_rs.at[i - 1],
            device_id=(lax.rem(z + i, n_z) * fold + y, t), device_id_type=MESH,
        )
        for i in range(1, n_z)
    ]
    for c in gz_copies:
        c.start()
    for k in range(2, n_z - 1):
        for h in range(2):
            hop(k, h)

    @pl.loop(0, n_blk)
    def _(i):
        at = pl.ds(pl.multiple_of(i * blk, blk), blk)
        gate = jax.nn.sigmoid(pg[:, at].astype(f32))
        d_glu = d_glu_s[at, :].T
        out_v[:, at] = (d_glu * gate).astype(jnp.bfloat16)
        out_g[:, at] = (d_glu * (pv[:, at].astype(f32) * gate) * (1.0 - gate)).astype(jnp.bfloat16)

    for c in gz_copies:
        c.wait()
    total = g_own[...]
    for i in range(n_z - 1):
        total = total + g_in[i]
    g_mid[...] = total
    gy = pltpu.make_async_remote_copy(
        src_ref=g_mid, dst_ref=g_yin, send_sem=gy_ss, recv_sem=gy_rs,
        device_id=(z * fold + other_y, t), device_id_type=MESH,
    )
    gy.start()
    for h in range(2):
        y_copies[n_z - 1][h].wait_recv()
        add_into(z, h, got_y)

        @pl.when(z > 0)
        def _():
            line_copy(z, h, True).wait_recv()
            add_into(z, h, got_r)

        @pl.when(z < n_z - 1)
        def _():
            line_copy(z, h, False).wait_recv()
            add_into(z, h, got_l)

    low_swap.wait()
    own = z * fold + y
    out_w[:top, :] = term[own, :top, :] * scale
    out_w[top:, :] = (term[own, top:, :] + low_y[...]) * scale
    gy.wait()
    out_t[...] = ((g_mid[...] + g_yin[...]) * scale)[:n_taps]
    for k in range(n_z):
        for h in range(2):
            y_copies[k][h].wait_send()

    @pl.when(s > 0)
    def _():
        halo.wait_send()

    for k in range(n_z - 1):
        d = dest[k]

        @pl.when(d > z)
        def _():
            for h in range(2):
                line_copy(d, h, True).wait_send()
            low_copy(d, True).wait_send()

        @pl.when(d < z)
        def _():
            for h in range(2):
                line_copy(d, h, False).wait_send()
            low_copy(d, False).wait_send()


def fused(n_sp, n_tp, proj_value, proj_gate, conv_saved, conv_taps, norm_gain, out_weight, cotangent):
    fold = 2
    n_z = n_sp // fold
    rows, width = cotangent.shape
    ch = conv_saved.shape[1]
    n_taps = conv_taps.shape[0]
    part = width // n_sp
    low = low_rows(ch)
    top = ch - low
    dma = pltpu.SemaphoreType.DMA
    V = pltpu.VMEM
    bf = jnp.bfloat16
    vm = pl.BlockSpec(memory_space=pltpu.VMEM)
    hb = pl.BlockSpec(memory_space=pl.ANY)
    grad_value, grad_gate, grad_weight, grad_taps = pl.pallas_call(
        functools.partial(kernel, n_sp, n_tp, fold),
        out_shape=(
            jax.ShapeDtypeStruct((ch, rows), bf),
            jax.ShapeDtypeStruct((ch, rows), bf),
            jax.ShapeDtypeStruct((ch, part), f32),
            jax.ShapeDtypeStruct((n_taps, ch), f32),
        ),
        in_specs=[hb, hb, vm, vm, vm, hb, hb],
        out_specs=[vm] * 4,
        scratch_shapes=[
            V((ch, rows), bf), V((ch, rows), bf), V((ch, width), bf), V((width, rows), bf), dma((4,)),
            V((ch, 128), f32), V((rows, ch), f32), V((rows, ch), f32),
            V((ch, rows), bf), V((ch, rows), f32), V((rows + 32, ch), f32), V((8, rows + 32, ch), f32),
            V((8, rows), f32), V((8, rows), f32),
            V((n_sp, ch, part), f32), V((n_z, top, part), f32), V((n_z, top, part), f32),
            V((n_z, top, part), f32),
            V((n_z, fold, low, part), f32), V((n_z, fold, low, part), f32), V((low, part), f32),
            V((8, rows), f32), V((n_tp - 1, 8, rows), f32), V((8, rows), f32), V((n_tp - 1, 8, rows), f32),
            V((n_taps, 8, ch), f32), V((32, ch), f32), V((32, ch), f32), V((n_z - 1, 32, ch), f32),
            V((32, ch), f32), V((n_taps, 8, ch), f32),
            dma((n_tp - 1,)), dma((n_tp - 1,)), dma((n_tp - 1,)), dma((n_tp - 1,)),
            *[dma((2 * n_z,))] * 6,
            dma((n_z,)), dma((n_z,)), dma((n_z,)), dma((n_z,)), dma, dma,
            dma, dma, dma((n_z - 1,)), dma((n_z - 1,)), dma, dma,
        ],
        compiler_params=pltpu.CompilerParams(
            collective_id=0, has_side_effects=True, vmem_limit_bytes=60 * 1024 * 1024
        ),
    )(
        proj_value.T, proj_gate.T, conv_saved.T, conv_taps, norm_gain, out_weight,
        cotangent.T,
    )
    results = (grad_value, grad_gate, grad_weight, grad_taps)
    grad_value, grad_gate, grad_weight, grad_taps = pl.pallas_call(
        finish,
        out_shape=tuple(jax.ShapeDtypeStruct(r.shape, r.dtype) for r in results),
        in_specs=[hb] * 4,
        out_specs=[hb] * 4,
        scratch_shapes=[V(r.shape, r.dtype) for r in results] + [dma((8,))],
        compiler_params=pltpu.CompilerParams(vmem_limit_bytes=60 * 1024 * 1024),
    )(*results)
    return grad_value.T, grad_gate.T, grad_weight, grad_taps


def passed_along(block, axis, distance):
    devices = range(lax.axis_size(axis))
    route = [(i - distance, i) for i in devices if i - distance in devices]
    return lax.ppermute(block, axis, route)


def local(proj_value, proj_gate, conv_saved, conv_taps, norm_gain, out_weight, cotangent):
    model_width = cotangent.shape[1]
    tok_rows = cotangent.shape[0]
    tap_count = conv_taps.shape[0]
    overhang = tap_count - 1
    grad_scale = 1.0 / math.sqrt(tok_rows * lax.axis_size("sp"))
    conv_f = conv_saved.astype(jnp.float32)
    totals = lax.psum((jnp.sum(conv_f, axis=1), jnp.sum(conv_f * conv_f, axis=1)), "tp")
    row_mean = totals[0] / model_width
    row_var = totals[1] / model_width - row_mean * row_mean
    inv_std = lax.rsqrt(row_var + norm_eps)
    centered = (conv_f - row_mean[:, None]) * inv_std[:, None]
    gain_f = norm_gain.astype(jnp.float32)
    normed = centered * gain_f
    gate_norm = jax.nn.sigmoid(normed)
    activated = (normed * gate_norm).astype(jnp.bfloat16)
    contract_rows = (((0,), (0,)), ((), ()))
    whole_term = lax.dot_general(
        cotangent, activated, contract_rows, preferred_element_type=jnp.float32
    )
    shard_grad = lax.psum_scatter(whole_term, "sp", scatter_dimension=0, tiled=True)
    grad_out_weight = shard_grad.T * grad_scale
    d_act = lax.dot_general(
        cotangent, out_weight, (((1,), (1,)), ((), ())), preferred_element_type=jnp.float32
    )
    d_hat = d_act * gate_norm * (1.0 + normed * (1.0 - gate_norm)) * gain_f
    moments = lax.psum((jnp.sum(d_hat, axis=1), jnp.sum(d_hat * centered, axis=1)), "tp")
    first = moments[0] / model_width
    second = moments[1] / model_width
    d_conv = inv_std[:, None] * (d_hat - first[:, None] - centered * second[:, None])
    ahead = passed_along(d_conv[:overhang], "sp", -1)
    extended = jnp.concatenate([d_conv, ahead], axis=0)
    gate_proj = jax.nn.sigmoid(proj_gate.astype(jnp.float32))
    gated = proj_value.astype(jnp.float32) * gate_proj
    taps_f = conv_taps.astype(jnp.float32)
    d_glu = jnp.zeros_like(d_conv)
    tap_rows = []
    for offset in range(tap_count):
        shifted = extended[overhang - offset : overhang - offset + tok_rows]
        d_glu = d_glu + taps_f[offset] * shifted
        tap_rows.append(jnp.sum(gated * shifted, axis=0))
    grad_taps = lax.psum(jnp.stack(tap_rows), "sp") * grad_scale
    grad_value = (d_glu * gate_proj).astype(jnp.bfloat16)
    grad_gate = (d_glu * gated * (1.0 - gate_proj)).astype(jnp.bfloat16)
    return (grad_value, grad_gate, grad_out_weight, grad_taps)


def solution(mesh):
    in_specs = (
        P("sp", "tp"),
        P("sp", "tp"),
        P("sp", "tp"),
        P(None, "tp"),
        P("tp"),
        P("tp", None),
        P("sp", None),
    )
    out_specs = (P("sp", "tp"), P("sp", "tp"), P("tp", "sp"), P(None, "tp"))
    n_sp, n_tp = mesh.shape["sp"], mesh.shape["tp"]

    def step(*args):
        rows, width = args[6].shape
        ch, n_taps = args[2].shape[1], args[3].shape[0]
        small = n_sp % 2 == 0 and 4 <= n_sp <= 8 and width % n_sp == 0 and n_tp > 1
        if small and rows % 128 == 0 and rows >= 128 and ch % 8 == 0 and 24 < n_taps <= 31:
            return fused(n_sp, n_tp, *args)
        return local(*args)

    return jax.shard_map(step, mesh=mesh, in_specs=in_specs, out_specs=out_specs, check_vma=False)
```
